32 devices in a mesh: sp: 8 (over z, x), tp: 4 (over y, core).
Axes of the slice: x: 2, y: 2, z: 4, core: 2. Of those that a mesh axis runs over, the one named last changes fastest.
Arguments:
- queries: bfloat16 [2560, 1024], P('sp', 'tp'), may hold values from -6.6 to 6.6
- key_matrix: bfloat16 [2560, 256], P('sp', 'tp'), may hold values from -6.6 to 6.6
- values: bfloat16 [2560, 256], P('sp', 'tp'), may hold values from -6 to 6
- query_gain: float32 [64], replicated, may hold values from 0.19 to 8
- key_norm_gain: float32 [64], replicated, may hold values from 0.19 to 8
- head_gain: float32 [1024], P('tp'), may hold values from 0.1 to 1.9
- out_proj: bfloat16 [1024, 2048], replicated, may hold values from -0.1875 to 0.1875
- residual: bfloat16 [2560, 2048], P('sp'), may hold values from -6 to 6
- ffn_gain: float32 [2048], replicated, may hold values from 0.1 to 1.9
- routes: int32 [2560, 4], P('sp'), may hold values from 0 to 31, all different within a row; in each aligned block of 320 rows (0 to 319, 320 to 639, ...) at most 80 rows name the same one
- route_weights: float32 [2560, 4], P('sp'), may hold values from 0.2 to 1
- expert_gate: bfloat16 [32, 2048, 512], P(('sp', 'tp')), may hold values from -0.125 to 0.125
- expert_up: bfloat16 [32, 2048, 512], P(('sp', 'tp')), may hold values from -0.125 to 0.125
- expert_down: bfloat16 [32, 512, 2048], P(('sp', 'tp')), may hold values from -0.25 to 0.25
- shared_gate: bfloat16 [2048, 512], P(None, 'tp'), may hold values from -0.125 to 0.125
- shared_up: bfloat16 [2048, 512], P(None, 'tp'), may hold values from -0.125 to 0.125
- shared_down: bfloat16 [512, 2048], P('tp'), may hold values from -0.25 to 0.25
Outputs:
- layer_out: bfloat16 [2560, 2048], P(('sp', 'tp'))
The draws below stay inside these ranges and needn't reach their ends.
Inputs may be any that keep to these rules, and one draw needn't show every extreme that they name: `routes`: each row names 4 different experts; in each aligned block of 320 rows (the tokens of one index of sp) no expert is named more than 80 times, a bound that some block reaches.
All inputs are finite; a program needn't handle non-finite values.
Results may differ from the reference program's by a relative error of at most 0.019.
The reference program's roundings to bfloat16 on the way count: a program that leaves them out, or rounds other values in their place, can miss the bound.
Values may be sent and summed in bfloat16 or wider, within the bound.
A program may use at most 128 MiB of HBM per device.

```python
import math
import jax
import jax.numpy as jnp
import numpy as np
from jax import lax

D = 2048
HEAD_SIZE = 64
QUERY_HEADS = 16
KEY_VALUE_HEADS = 4
FF = 512
SFF = 512
TOPK = 4
GRID_W = 64
TOK_DEV = 320
SEQUENCE_TOKENS = 2560
EXPERTS = 32
CAP = 80
N_SP = 8
N_TP = 4


def plant_pair(key):
    unrotated_query = jnp.clip(jax.random.normal(jax.random.fold_in(key, 11), (SEQUENCE_TOKENS, QUERY_HEADS * HEAD_SIZE), jnp.float32), -6.0, 6.0)
    unrotated_key = jnp.clip(jax.random.normal(jax.random.fold_in(key, 12), (SEQUENCE_TOKENS, KEY_VALUE_HEADS * HEAD_SIZE), jnp.float32), -6.0, 6.0)
    return (unrotated_query, unrotated_key)


def draw_queries(key, part):
    return plant_pair(key)[0].astype(jnp.bfloat16)


def draw_key_matrix(key, part):
    return plant_pair(key)[1].astype(jnp.bfloat16)


def gain_draw(key, salt):
    folded = jax.random.fold_in(key, salt)
    return 1.0 + 0.18 * jnp.clip(jax.random.normal(folded, (HEAD_SIZE,), jnp.float32), -4.5, 4.5)


def draw_query_gain(key, part):
    return gain_draw(key, 21)


def draw_key_norm_gain(key, part):
    return gain_draw(key, 22)


def block_scale(key, dims, cuts, smallest, top_value):
    factor_of, own = 1.0, jax.random.fold_in(key, 6)
    for axis_at, parts in cuts:
        heights = jnp.exp(jax.random.uniform(jax.random.fold_in(own, axis_at), (parts,), jnp.float32, smallest / len(cuts), top_value / len(cuts)))
        factor_of = factor_of * jnp.repeat(heights, dims[axis_at] // parts).reshape([-1 if axis == axis_at else 1 for axis in range(len(dims))])
    return factor_of


def routed_block(own_key, own, number, rows, amount, top, limit, skew):
    order = jax.random.permutation(own_key, amount)
    packed, common = portions_of(amount, rows * top, limit, skew, True), portions_of(amount, rows * top, limit, skew, False)
    places = jnp.arange(amount)

    def named(tallies, rotation):
        used = int((tallies > 0).sum())
        fixed = max(1, used // 4)
        passed = fixed + (places - fixed + rotation * (used - fixed)) % max(1, amount - fixed)
        return jnp.zeros((amount,), jnp.int32).at[order[jnp.where(places < fixed, places, passed)]].set(jnp.asarray(tallies, jnp.int32))

    tallies = jnp.where(number % 4 == 0, named(packed, number // 4), named(common, number - number // 4 - 1))
    mixed = jax.random.permutation(jax.random.fold_in(own, 3), amount)
    source_of, receiver = mixed[0:amount // 2 * 2:2], mixed[1:amount // 2 * 2:2]
    room = jnp.minimum(tallies[source_of] - 1, limit - tallies[receiver]) // 2
    room = jnp.where((source_of == order[0]) | (receiver == order[0]) | (tallies[receiver] == 0), 0, jnp.maximum(room, 0))
    passed = jax.random.randint(jax.random.fold_in(own, 4), (amount // 2,), 0, 1 << 20) % (room + 1)
    tallies = tallies.at[source_of].add(-passed).at[receiver].add(passed)
    items = jnp.searchsorted(jnp.cumsum(tallies), jnp.arange(rows * top), side="right").astype(jnp.int32)
    grid = items.reshape(top, rows).T
    grid = grid[jax.random.permutation(jax.random.fold_in(own, 1), rows)]
    rotation = jax.random.randint(jax.random.fold_in(own, 2), (rows, 1), 0, top)
    return jnp.take_along_axis(grid, (jnp.arange(top)[None, :] + rotation) % top, axis=1)


def portions_of(number_of, total, limit, slope, full):
    weights = [(1 << 20) // math.isqrt(rank ** slope) + 1 for rank in range(1, number_of + 1)]
    largest = limit if full else min(limit, max(-(-total // number_of), total * weights[0] // sum(weights)))
    least = 1 if total - largest >= number_of - 1 else 0
    given, surplus = [largest] + [least] * (number_of - 1), total - largest - least * (number_of - 1)
    while surplus > 0:
        free = [i for i in range(1, number_of) if given[i] < largest] or [i for i in range(1, number_of) if given[i] < limit]
        whole, left = sum([weights[i] for i in free]), surplus
        for i in free:
            addition = min(limit - given[i], max(1, left * weights[i] // whole), surplus)
            given[i] = given[i] + addition
            surplus = surplus - addition
    return np.array(given)


def normal_values(rng, dims, spread, reach, cuts=(), kind=jnp.bfloat16):
    values = spread * jax.random.normal(rng, dims, jnp.float32)
    if cuts:
        values = values * block_scale(rng, dims, cuts, -0.22, 0.18)
    return jnp.clip(values, -reach, reach).astype(kind)


def setup_inputs(seed: int = 0) -> dict:
    seeds = jax.random.split(jax.random.key(seed), 18)
    queries = draw_queries(jax.random.fold_in(seeds[17], 71), 0)
    key_matrix = draw_key_matrix(jax.random.fold_in(seeds[17], 71), 0)
    values = normal_values(seeds[2], (SEQUENCE_TOKENS, KEY_VALUE_HEADS * HEAD_SIZE), 1.0, 6.0, ((0, 8), (1, 4)))
    query_gain = draw_query_gain(jax.random.fold_in(seeds[17], 71), 0)
    key_norm_gain = draw_key_norm_gain(jax.random.fold_in(seeds[17], 71), 0)
    head_gain = jnp.clip(1.0 + 0.18 * jax.random.normal(seeds[5], (QUERY_HEADS * HEAD_SIZE,), jnp.float32), 0.1, 1.9)
    out_proj = normal_values(seeds[6], (QUERY_HEADS * HEAD_SIZE, D), (QUERY_HEADS * HEAD_SIZE) ** -0.5, 0.1875)
    residual = normal_values(seeds[7], (SEQUENCE_TOKENS, D), 1.0, 6.0, ((0, 8),))
    ffn_gain = jnp.clip(1.0 + 0.18 * jax.random.normal(seeds[8], (D,), jnp.float32), 0.1, 1.9)
    routes_keys = jax.random.split(jax.random.fold_in(seeds[9], 1), SEQUENCE_TOKENS // TOK_DEV)
    routes_turns = jax.random.permutation(jax.random.fold_in(seeds[9], 3), SEQUENCE_TOKENS // TOK_DEV)
    routes = jax.vmap(lambda own, number: routed_block(jax.random.fold_in(seeds[9], 2), own, number, TOK_DEV, EXPERTS, TOPK, CAP, 1))(routes_keys, routes_turns).reshape((SEQUENCE_TOKENS, TOPK))
    route_weights = jnp.clip(0.2 + 0.8 * jax.random.uniform(seeds[10], (SEQUENCE_TOKENS, TOPK), jnp.float32) ** block_scale(seeds[10], (SEQUENCE_TOKENS, TOPK), ((0, 8),), -0.2, 0.2), 0.2, 1.0)
    expert_gate = normal_values(seeds[11], (EXPERTS, D, FF), D ** -0.5, 0.125, ((0, 32),))
    expert_up = normal_values(seeds[12], (EXPERTS, D, FF), D ** -0.5, 0.125, ((0, 32),))
    expert_down = normal_values(seeds[13], (EXPERTS, FF, D), FF ** -0.5, 0.25, ((0, 32),))
    shared_gate = normal_values(seeds[14], (D, SFF), D ** -0.5, 0.125, ((1, 4),))
    shared_up = normal_values(seeds[15], (D, SFF), D ** -0.5, 0.125, ((1, 4),))
    shared_down = normal_values(seeds[16], (SFF, D), SFF ** -0.5, 0.25, ((0, 4),))
    return dict(queries=queries, key_matrix=key_matrix, values=values, query_gain=query_gain, key_norm_gain=key_norm_gain, head_gain=head_gain, out_proj=out_proj, residual=residual, ffn_gain=ffn_gain, routes=routes, route_weights=route_weights, expert_gate=expert_gate, expert_up=expert_up, expert_down=expert_down, shared_gate=shared_gate, shared_up=shared_up, shared_down=shared_down)


EPS = 1e-06
THETA = 10000.0

def final_norm(field, gain):
    mean_sq = lax.optimization_barrier(jnp.mean(field * field, axis=-1, keepdims=True))
    return field * lax.rsqrt(mean_sq + EPS) * gain

def grid_tables(positions, sequence_total):
    grid_rows = sequence_total // GRID_W
    row_pos = (positions // GRID_W - grid_rows // 2).astype(jnp.float32)
    col_pos = (positions % GRID_W - GRID_W // 2).astype(jnp.float32)
    quarter = HEAD_SIZE // 4
    inverse = THETA ** (-jnp.arange(quarter, dtype=jnp.float32) / quarter)
    angles = jnp.concatenate([row_pos[:, None] * inverse, col_pos[:, None] * inverse], axis=1)
    return (jnp.cos(angles), jnp.sin(angles))

def apply_rotary(field, cosine_table, sine_table):
    row_count, head_count = (field.shape[0], field.shape[1])
    quarter = HEAD_SIZE // 4
    pieces = field.reshape(row_count, head_count, 2, 2, quarter)
    front_half = pieces[:, :, :, 0, :].reshape(row_count, head_count, 2 * quarter)
    back_half = pieces[:, :, :, 1, :].reshape(row_count, head_count, 2 * quarter)
    cos_wide = cosine_table[:, None, :]
    sin_wide = sine_table[:, None, :]
    new_front = (front_half * cos_wide - back_half * sin_wide).reshape(row_count, head_count, 2, 1, quarter)
    new_back = (front_half * sin_wide + back_half * cos_wide).reshape(row_count, head_count, 2, 1, quarter)
    return jnp.concatenate([new_front, new_back], axis=3).reshape(row_count, head_count, HEAD_SIZE)

def reference(queries, key_matrix, values, query_gain, key_norm_gain, head_gain, out_proj, residual, ffn_gain, routes, route_weights, expert_gate, expert_up, expert_down, shared_gate, shared_up, shared_down):
    sequence_total = SEQUENCE_TOKENS
    positions = jnp.arange(sequence_total, dtype=jnp.int32)
    cosine_table, sine_table = grid_tables(positions, sequence_total)
    rotated_query = apply_rotary(final_norm(queries.astype(jnp.float32).reshape(sequence_total, QUERY_HEADS, HEAD_SIZE), query_gain), cosine_table, sine_table).astype(jnp.bfloat16)
    rotated_key = apply_rotary(final_norm(key_matrix.astype(jnp.float32).reshape(sequence_total, KEY_VALUE_HEADS, HEAD_SIZE), key_norm_gain), cosine_table, sine_table).astype(jnp.bfloat16)
    group_width = QUERY_HEADS // KEY_VALUE_HEADS
    block_length = 64
    query_block_list = rotated_query.reshape(sequence_total // block_length, block_length, KEY_VALUE_HEADS, group_width, HEAD_SIZE)
    key_wide = rotated_key.astype(jnp.float32)
    value_expanded = values.reshape(sequence_total, KEY_VALUE_HEADS, HEAD_SIZE).astype(jnp.float32)
    score_scale = HEAD_SIZE ** (-0.5)

    def attend(query_block):
        scores = jnp.einsum('qkgd,skd->kgqs', query_block.astype(jnp.float32), key_wide) * score_scale
        row_max = lax.optimization_barrier(jnp.max(scores, axis=-1, keepdims=True))
        expo_terms = jnp.exp(scores - row_max)
        weights = lax.optimization_barrier(expo_terms.astype(jnp.bfloat16)).astype(jnp.float32)
        mixed_vals = jnp.einsum('kgqs,skd->qkgd', weights, value_expanded)
        denominator = jnp.moveaxis(lax.optimization_barrier(jnp.sum(expo_terms, axis=-1)), -1, 0)
        return mixed_vals / denominator[..., None]
    attended = lax.map(attend, query_block_list).reshape(sequence_total, QUERY_HEADS, HEAD_SIZE)
    head_out = final_norm(attended, head_gain.reshape(QUERY_HEADS, HEAD_SIZE)).astype(jnp.bfloat16).reshape(sequence_total, QUERY_HEADS * HEAD_SIZE)
    hidden = (residual.astype(jnp.float32) + jnp.dot(head_out, out_proj, preferred_element_type=jnp.float32)).astype(jnp.bfloat16)
    normed = final_norm(hidden.astype(jnp.float32), ffn_gain).astype(jnp.bfloat16)
    flat_expert = routes.reshape(-1).astype(jnp.int32)
    entries = flat_expert.shape[0]
    order_ids = jnp.argsort(flat_expert, stable=True).astype(jnp.int32)
    sorted_expert = flat_expert[order_ids]
    counts_per = jnp.bincount(flat_expert, length=EXPERTS).astype(jnp.int32)
    starts = (jnp.cumsum(counts_per) - counts_per).astype(jnp.int32)
    rank_ids = (jnp.arange(entries, dtype=jnp.int32) - starts[sorted_expert]).astype(jnp.int32)
    slot_table = jnp.full((EXPERTS, N_SP * CAP), entries, jnp.int32).at[sorted_expert, rank_ids].set(order_ids)
    entry_weight = jnp.concatenate([route_weights.reshape(-1), jnp.zeros((1,), jnp.float32)])
    entry_token = jnp.concatenate([jnp.arange(entries, dtype=jnp.int32) // TOPK, jnp.zeros((1,), jnp.int32)])
    slice_width = SFF // N_TP
    result = hidden.astype(jnp.float32)
    for owner in range(N_TP):
        col_start = owner * slice_width
        gate_part = jnp.dot(normed, shared_gate[:, col_start:col_start + slice_width], preferred_element_type=jnp.float32)
        up_part = jnp.dot(normed, shared_up[:, col_start:col_start + slice_width], preferred_element_type=jnp.float32)
        inner_act = (jax.nn.silu(gate_part) * up_part).astype(jnp.bfloat16)
        partial_sum = jnp.dot(inner_act, shared_down[col_start:col_start + slice_width, :], preferred_element_type=jnp.float32)

        def add_expert(total_acc, local_index, owner=owner):
            expert = local_index * N_TP + owner
            entry_ids = slot_table[expert]
            token_ids = entry_token[entry_ids]
            rows_in = normed[token_ids]
            gate_out = jnp.dot(rows_in, expert_gate[expert], preferred_element_type=jnp.float32)
            up_out = jnp.dot(rows_in, expert_up[expert], preferred_element_type=jnp.float32)
            expert_inner = (jax.nn.silu(gate_out) * up_out).astype(jnp.bfloat16)
            produced = jnp.dot(expert_inner, expert_down[expert], preferred_element_type=jnp.float32).astype(jnp.bfloat16)
            weighted = produced.astype(jnp.float32) * entry_weight[entry_ids][:, None]
            return (total_acc.at[token_ids].add(weighted), None)
        partial_sum, _ = lax.scan(add_expert, partial_sum, jnp.arange(EXPERTS // N_TP, dtype=jnp.int32))
        result = result + lax.optimization_barrier(partial_sum.astype(jnp.bfloat16)).astype(jnp.float32)
    return result.astype(jnp.bfloat16)
```

```python
import jax
import jax.numpy as jnp
from jax import lax
from jax.experimental import pallas as pl
from jax.experimental.pallas import tpu as pltpu
from jax.sharding import PartitionSpec as P

HEAD_SIZE = 64
GRID_W = 64


EPS = 1e-06
THETA = 10000.0


def final_norm(field, gain):
    mean_sq = jnp.mean(field * field, axis=-1, keepdims=True)
    return field * lax.rsqrt(mean_sq + EPS) * gain


def grid_tables(positions, sequence_total):
    grid_rows = sequence_total // GRID_W
    row_pos = (positions // GRID_W - grid_rows // 2).astype(jnp.float32)
    col_pos = (positions % GRID_W - GRID_W // 2).astype(jnp.float32)
    quarter = HEAD_SIZE // 4
    inverse = THETA ** (-jnp.arange(quarter, dtype=jnp.float32) / quarter)
    angles = jnp.concatenate([row_pos[:, None] * inverse, col_pos[:, None] * inverse], axis=1)
    return (jnp.cos(angles), jnp.sin(angles))


def apply_rotary(field, cosine_table, sine_table):
    row_count, head_count = (field.shape[0], field.shape[1])
    quarter = HEAD_SIZE // 4
    pieces = field.reshape(row_count, head_count, 2, 2, quarter)
    front_half = pieces[:, :, :, 0, :].reshape(row_count, head_count, 2 * quarter)
    back_half = pieces[:, :, :, 1, :].reshape(row_count, head_count, 2 * quarter)
    cos_wide = cosine_table[:, None, :]
    sin_wide = sine_table[:, None, :]
    new_front = (front_half * cos_wide - back_half * sin_wide).reshape(
        row_count, head_count, 2, 1, quarter
    )
    new_back = (front_half * sin_wide + back_half * cos_wide).reshape(
        row_count, head_count, 2, 1, quarter
    )
    return jnp.concatenate([new_front, new_back], axis=3).reshape(row_count, head_count, HEAD_SIZE)


def exchange(block, axis, call_id, gather):
    count = lax.axis_size(axis)
    if count == 1:
        return block[None] if gather else block
    shape = (count,) + block.shape if gather else block.shape

    def kernel(in_ref, out_ref, send_sems, recv_sems, own_sem):
        me = lax.axis_index(axis)
        barrier = pltpu.get_barrier_semaphore()
        for step in range(1, count):
            pl.semaphore_signal(
                barrier,
                inc=1,
                device_id={axis: lax.rem(me + step, count)},
                device_id_type=pl.DeviceIdType.MESH,
            )
        own = pltpu.make_async_copy(in_ref if gather else in_ref.at[me], out_ref.at[me], own_sem)
        own.start()
        pl.semaphore_wait(barrier, count - 1)
        copies = []
        for step in range(1, count):
            peer = lax.rem(me + step, count)
            copy = pltpu.make_async_remote_copy(
                src_ref=in_ref if gather else in_ref.at[peer],
                dst_ref=out_ref.at[me],
                send_sem=send_sems.at[step],
                recv_sem=recv_sems.at[step],
                device_id={axis: peer},
                device_id_type=pl.DeviceIdType.MESH,
            )
            copy.start()
            copies.append(copy)
        own.wait()
        for copy in copies:
            copy.wait()

    return pl.pallas_call(
        kernel,
        out_shape=jax.ShapeDtypeStruct(shape, block.dtype),
        in_specs=[pl.BlockSpec(memory_space=pltpu.VMEM)],
        out_specs=pl.BlockSpec(memory_space=pltpu.VMEM),
        scratch_shapes=[
            pltpu.SemaphoreType.DMA((count,)),
            pltpu.SemaphoreType.DMA((count,)),
            pltpu.SemaphoreType.DMA,
        ],
        compiler_params=pltpu.CompilerParams(collective_id=call_id, has_side_effects=True),
        name="exchange_%d" % call_id,
    )(block)


def key_block_rows(piece_rows):
    return max((width for width in range(1, 2049) if piece_rows % width == 0))


MESH = pl.DeviceIdType.MESH
COLUMNS = 512
FLIPS = ((1, 2), (1, 3), (0, 2), (0, 3), (1, 0), (1, 1), (0, 1))
TP_FLIPS = (2, 3, 1)


def remote(source, target, send_sem, recv_sem, device):
    return pltpu.make_async_remote_copy(
        src_ref=source,
        dst_ref=target,
        send_sem=send_sem,
        recv_sem=recv_sem,
        device_id=device,
        device_id_type=MESH,
    )


def whole_layer(
    queries_t,
    packet,
    gain,
    ffn_gain,
    residual,
    weights,
    tokens,
    capacity,
    topk,
    width,
    tp_count,
    call_id,
):
    count = lax.axis_size("sp")
    planes = count // width
    group = width * tp_count
    span = queries_t.shape[1]
    heads = gain.shape[0]
    features = heads * HEAD_SIZE
    model = residual.shape[1]
    quarter = model // tp_count
    rows_each = tokens // tp_count
    chunk = 256
    lane_groups = -(-tokens // 128)
    lanes = 128 * lane_groups
    table_rows = packet.shape[0] - tokens
    table_step = table_rows // lane_groups
    slots = group * capacity
    out_proj, gate_w, up_w, down_w, shared_gate, shared_up, shared_down = weights
    hidden_units = gate_w.shape[1]
    shared_units = shared_gate.shape[1]
    pair = width * capacity
    half = tokens // 2
    bf16, f32 = jnp.bfloat16, jnp.float32

    def kernel(
        q_ref, own_ref, gain_ref, ffn_ref, resid_ref, wo_hbm, wg_hbm, wu_hbm, wd_hbm,
        sg_hbm, su_hbm, sd_hbm, out_ref,
        kv, top, norm, acc, tri, ranks, scales, sel, sel_t, rblk, hblk, rpack, hpack,
        xr, xh, hs, ns, ret, rr, passed, arrived, base, fin, hg, own_hid, si, sdq,
        res, wo, wg, wu, wd, sg, su,
        w_sem, k_sem, kz_send, kx_send, k_recv,
        rz_send, rz_recv, ri_send, ri_recv, hz_send, hz_recv, hi_send, hi_recv,
        hg_send, hg_recv, sd_send, sd_recv, si_send, si_recv,
        rt_send, rt_recv, zr_send, zr_recv, f_send, f_recv,
    ):
        me, t = lax.axis_index("sp"), lax.axis_index("tp")
        z, x = me // width, me % width
        p = x * tp_count + t
        side = z // 2
        inner = jnp.where((z == 1) | (z == 2), 1, 0)

        def nearest(k):
            near = k + inner * (1 - 2 * k) if k < 2 else k
            return near + side * (planes - 1 - 2 * near)

        def mate(dx, dt):
            x2 = 1 - x if dx else x
            t2 = t
            if dt & 2:
                t2 = t2 + 2 * (1 - 2 * (t // 2))
            if dt & 1:
                t2 = t2 + (1 - 2 * (t % 2))
            return x2, t2

        def at(plane, x2, t2):
            return {"sp": plane * width + x2, "tp": t2}

        arrived[...] = jnp.zeros(arrived.shape, bf16)
        barrier = pltpu.get_barrier_semaphore()
        for dx, dt in FLIPS:
            pl.semaphore_signal(barrier, inc=1, device_id=at(z, *mate(dx, dt)), device_id_type=MESH)
        for step in range(1, planes):
            pl.semaphore_signal(
                barrier, inc=1, device_id=at(lax.rem(z + step, planes), x, t), device_id_type=MESH
            )

        def columns(index, size):
            return pl.ds(pl.multiple_of(index * size, 128), size)

        kept = pltpu.make_async_copy(own_ref, kv.at[me], k_sem.at[0])
        kept.start()
        mine = pltpu.make_async_copy(resid_ref.at[:, columns(t, quarter)], rblk.at[z], k_sem.at[1])
        mine.start()
        loads = [
            pltpu.make_async_copy(source, target, w_sem.at[i])
            for i, (source, target) in enumerate(
                [
                    (wo_hbm, wo), (wg_hbm, wg), (wu_hbm, wu), (wd_hbm, wd),
                    (sg_hbm, sg), (su_hbm, su), (resid_ref, res),
                ]
            )
        ]
        for load in loads:
            load.start()
        before = lax.broadcasted_iota(jnp.int32, (lanes, lanes), 0)
        after = lax.broadcasted_iota(jnp.int32, (lanes, lanes), 1)
        tri[...] = jnp.where(before < after, 1.0, 0.0).astype(bf16)
        top[...] = jnp.full(top.shape, -1e30, f32)
        norm[...] = jnp.zeros(norm.shape, f32)
        acc[...] = jnp.zeros(acc.shape, f32)
        kept.wait()
        mine.wait()
        pl.semaphore_wait(barrier, len(FLIPS) + planes - 1)

        def along(step):
            return remote(
                own_ref, kv.at[me], kz_send.at[step], k_recv.at[me],
                at(lax.rem(z + step, planes), x, t),
            )

        def came(slot):
            return remote(own_ref, kv.at[slot], kz_send.at[0], k_recv.at[slot], at(z, 1 - x, t))

        def across(plane):
            slot = plane * width + x
            return remote(kv.at[slot], kv.at[slot], kx_send.at[plane], k_recv.at[slot], at(z, 1 - x, t))

        def z_hop(blk, b, up, ssem, rsem):
            return remote(
                blk.at[b], blk.at[b], ssem.at[up, b], rsem.at[b],
                at(z + (1 if up else -1), x, t),
            )

        def goes(b, up):
            return (b <= z) & (z < planes - 1) if up else (b >= z) & (z > 0)

        def forward(blk, b, ssem, rsem):
            for up in (1, 0):
                @pl.when(goes(b, up))
                def _():
                    z_hop(blk, b, up, ssem, rsem).start()

        def landed(b, wide, dst, x2, t2):
            return dst.at[b * width + x2, :, columns(t2, wide)]

        def deal_copy(b, pack, dst, wide, ssem, rsem, i):
            x2, t2 = mate(*FLIPS[i])
            rows = pl.ds(pl.multiple_of((x2 * tp_count + t2) * capacity, 16), capacity)
            return remote(
                pack.at[b, rows], landed(b, wide, dst, x, t), ssem.at[b, i], rsem.at[b, i],
                at(z, x2, t2),
            )

        def deal_own(b, pack, dst, wide, rsem):
            rows = pl.ds(pl.multiple_of(p * capacity, 16), capacity)
            return pltpu.make_async_copy(
                pack.at[b, rows], landed(b, wide, dst, x, t), rsem.at[b, len(FLIPS)]
            )

        def deal(b, blk, pack, dst, wide, ssem, rsem):
            for start in range(0, slots, tokens):
                pack[b, start : start + tokens, :] = jnp.dot(
                    sel[b, start : start + tokens, 0:tokens], blk[b], preferred_element_type=f32
                ).astype(bf16)
            for i in range(len(FLIPS)):
                deal_copy(b, pack, dst, wide, ssem, rsem, i).start()
            deal_own(b, pack, dst, wide, rsem).start()

        def dealt(b, pack, dst, wide, ssem, rsem):
            for i in range(len(FLIPS)):
                x2, t2 = mate(*FLIPS[i])
                remote(
                    pack.at[b, 0:capacity], landed(b, wide, dst, x2, t2), ssem.at[b, i],
                    rsem.at[b, i], at(z, x2, t2),
                ).wait_recv()
            deal_own(b, pack, dst, wide, rsem).wait()

        resid_path = (rblk, rpack, xr, quarter, ri_send, ri_recv)
        heads_path = (hblk, hpack, xh, features, hi_send, hi_recv)

        def table(slot):
            return kv[slot, tokens : tokens + table_rows, :].astype(f32)

        def index(b):
            rows = table(b * width + x)
            named = (lax.broadcasted_iota(jnp.int32, (group, 128), 0) + z * group).astype(f32)
            for j in range(lane_groups):
                hit = jnp.zeros((group, 128), f32)
                for k in range(topk):
                    row = rows[j * table_step + k : j * table_step + k + 1]
                    hit = jnp.where(row == named, 1.0, hit)
                ranks[0:group, 128 * j : 128 * j + 128] = hit
            member = ranks[0:group, :]
            rank = jnp.dot(member.astype(bf16), tri[...], preferred_element_type=f32)
            ranks[0:group, :] = jnp.where(member > 0.5, rank, -1.0)
            wanted = lax.broadcasted_iota(jnp.int32, (capacity, 128), 0).astype(f32)
            for e in range(group):
                for j in range(lane_groups):
                    row = ranks[e : e + 1, 128 * j : 128 * j + 128]
                    sel[b, e * capacity : (e + 1) * capacity, 128 * j : 128 * j + 128] = jnp.where(
                        row == wanted, 1.0, 0.0
                    ).astype(bf16)

        def weigh(slot, carry):
            rows = table(slot)
            mine_is = (z * group + p).astype(f32)
            amounts = []
            for j in range(lane_groups):
                hit = jnp.zeros((1, 128), f32)
                amount = jnp.zeros((1, 128), f32)
                for k in range(topk):
                    at_row = j * table_step + k
                    same = rows[at_row : at_row + 1] == mine_is
                    high = rows[at_row + topk : at_row + topk + 1]
                    low = rows[at_row + 2 * topk : at_row + 2 * topk + 1]
                    hit = jnp.where(same, 1.0, hit)
                    amount = jnp.where(same, high + low, amount)
                ranks[0:8, 128 * j : 128 * j + 128] = jnp.broadcast_to(hit, (8, 128))
                amounts.append(amount)
            member = ranks[0:8, :]
            rank = jnp.dot(member.astype(bf16), tri[...], preferred_element_type=f32)
            ranks[0:8, :] = jnp.where(member > 0.5, rank, -1.0)
            wanted = lax.broadcasted_iota(jnp.int32, (capacity, 128), 0).astype(f32)
            summed = jnp.zeros((capacity, 128), f32)
            for j in range(lane_groups):
                row = ranks[0:1, 128 * j : 128 * j + 128]
                summed = summed + jnp.where(row == wanted, amounts[j], 0.0)
            scales[slot] = jnp.broadcast_to(
                jnp.sum(summed, axis=1, keepdims=True), (capacity, 128)
            )
            return carry

        def absorb(slot):
            keys = kv[slot, 0:tokens, 0:HEAD_SIZE]
            vals_t = kv[slot, 0:tokens, HEAD_SIZE : 2 * HEAD_SIZE].T
            for start in range(0, span, chunk):
                part = pl.ds(start, chunk)
                scores = jnp.dot(keys, q_ref[:, part], preferred_element_type=f32)
                old = top[:, part]
                peak = jnp.maximum(old, jnp.max(scores, axis=0, keepdims=True))
                factor = jnp.exp(old - peak)
                terms = jnp.exp(scores - peak)
                norm[:, part] = norm[:, part] * factor + jnp.sum(terms, axis=0, keepdims=True)
                acc[:, part] = acc[:, part] * factor + jnp.dot(
                    vals_t, terms.astype(bf16), preferred_element_type=f32
                )
                top[:, part] = peak

        for step in range(1, planes):
            along(step).start()
        across(z).start()
        forward(rblk, z, rz_send, rz_recv)
        sd_copies = []
        for i, dt in enumerate(TP_FLIPS):
            _, t2 = mate(0, dt)
            copy = remote(
                sd_hbm.at[:, columns(t2, quarter)],
                sdq.at[pl.ds(pl.multiple_of(t * shared_units, 16), shared_units)],
                sd_send.at[i], sd_recv.at[i], at(z, x, t2),
            )
            sd_copies.append(copy)
        sd_own = pltpu.make_async_copy(
            sd_hbm.at[:, columns(t, quarter)],
            sdq.at[pl.ds(pl.multiple_of(t * shared_units, 16), shared_units)],
            sd_recv.at[len(TP_FLIPS)],
        )
        sd_own.start()
        index(z)
        deal(z, *resid_path)
        absorb(me)
        for k in range(1, planes):
            b, last = nearest(k), nearest(k - 1)
            came(b * width + x).wait_recv()
            across(b).start()
            index(b)
            z_hop(rblk, b, 0, rz_send, rz_recv).wait_recv()
            forward(rblk, b, rz_send, rz_recv)
            deal(b, *resid_path)
            came(last * width + (1 - x)).wait_recv()
            absorb(last * width + (1 - x))
            absorb(b * width + x)
        for copy in sd_copies:
            copy.start()
        last = nearest(planes - 1)
        came(last * width + (1 - x)).wait_recv()
        absorb(last * width + (1 - x))

        attended = acc[...] / norm[...]
        mean_sq = jnp.mean(attended * attended, axis=0, keepdims=True)
        rows = (attended * lax.rsqrt(mean_sq + EPS)).T
        for h in range(heads):
            hblk[z, :, h * HEAD_SIZE : (h + 1) * HEAD_SIZE] = (
                rows[h * tokens : (h + 1) * tokens] * gain_ref[h : h + 1, :]
            ).astype(bf16)

        forward(hblk, z, hz_send, hz_recv)
        deal(z, *heads_path)

        def gather(i):
            _, t2 = mate(0, TP_FLIPS[i])
            return remote(
                hblk.at[z], hg.at[:, columns(t, features)], hg_send.at[i], hg_recv.at[i],
                at(z, x, t2),
            )

        for i in range(len(TP_FLIPS)):
            gather(i).start()
        hg_own = pltpu.make_async_copy(
            hblk.at[z], hg.at[:, columns(t, features)], hg_recv.at[len(TP_FLIPS)]
        )
        hg_own.start()

        def pass_heads(k):
            b = nearest(k)
            z_hop(hblk, b, 0, hz_send, hz_recv).wait_recv()
            forward(hblk, b, hz_send, hz_recv)
            deal(b, *heads_path)

        def normalize(head_rows, resid_at):
            count_rows = head_rows.shape[0]
            squares = jnp.zeros((count_rows, 1), f32)
            for start in range(0, model, COLUMNS):
                part = slice(start, start + COLUMNS)
                field = jnp.dot(head_rows, wo[:, part], preferred_element_type=f32)
                field = (resid_at(part).astype(f32) + field).astype(bf16)
                hs[:, part] = field
                field = field.astype(f32)
                squares = squares + jnp.sum(field * field, axis=1, keepdims=True)
            inverse = lax.rsqrt(squares / model + EPS)
            for start in range(0, model, COLUMNS):
                part = slice(start, start + COLUMNS)
                ns[:, part] = (hs[:, part].astype(f32) * inverse * ffn_ref[:, part]).astype(bf16)

        def glu(gate_ref, up_ref):
            gate = jnp.dot(ns[...], gate_ref[...], preferred_element_type=f32)
            up = jnp.dot(ns[...], up_ref[...], preferred_element_type=f32)
            return (gate / (1.0 + jnp.exp(-gate)) * up).astype(bf16)

        def back_copy(b, j, i):
            x2, t2 = mate(*FLIPS[i])
            return remote(
                ret.at[b * width + x2, :, columns(t2, quarter)], rr.at[b, p],
                rt_send.at[b, i], rt_recv.at[b, i], at(z, x2, t2),
            )

        def back_own(b):
            return pltpu.make_async_copy(
                ret.at[b * width + x, :, columns(t, quarter)], rr.at[b, p],
                rt_recv.at[b, len(FLIPS)],
            )

        def expert(k):
            b = nearest(k)
            dealt(b, *resid_path[1:])
            dealt(b, *heads_path[1:])
            both = pl.ds(b * width, width)

            def resid_at(part):
                return xr[both, :, part].reshape(pair, COLUMNS)

            normalize(xh[both].reshape(pair, tp_count * features), resid_at)
            inner_rows = glu(wg, wu)
            scale = scales[both].reshape(pair, 128)[:, 0:1]
            for start in range(0, model, COLUMNS):
                part = slice(start, start + COLUMNS)
                made = jnp.dot(inner_rows, wd[:, part], preferred_element_type=f32) * scale
                ret[both, :, part] = made.astype(bf16).reshape(width, capacity, COLUMNS)
            for i in range(len(FLIPS)):
                back_copy(b, 0, i).start()
            back_own(b).start()

        def inner_copy(i):
            _, t2 = mate(0, TP_FLIPS[i])
            return remote(
                si.at[:, columns(t, shared_units)], si.at[:, columns(t, shared_units)],
                si_send.at[i], si_recv.at[i], at(z, x, t2),
            )

        def shared_inner():
            for i in range(len(TP_FLIPS)):
                _, t2 = mate(0, TP_FLIPS[i])
                remote(
                    hblk.at[z], hg.at[:, columns(t2, features)], hg_send.at[i], hg_recv.at[i],
                    at(z, x, t2),
                ).wait_recv()
            hg_own.wait()
            for start in (0, half):
                span_rows = slice(start, start + half)
                normalize(hg[span_rows, :], lambda part: res[span_rows, part])
                own_hid[span_rows, :] = hs[:, columns(t, quarter)]
                si[span_rows, columns(t, shared_units)] = glu(sg, su)
            for i in range(len(TP_FLIPS)):
                inner_copy(i).start()

        def shared_out():
            for i in range(len(TP_FLIPS)):
                _, t2 = mate(0, TP_FLIPS[i])
                remote(
                    si.at[:, columns(t, shared_units)], si.at[:, columns(t2, shared_units)],
                    si_send.at[i], si_recv.at[i], at(z, x, t2),
                ).wait_recv()
                remote(
                    sd_hbm.at[:, columns(t2, quarter)],
                    sdq.at[pl.ds(pl.multiple_of(t2 * shared_units, 16), shared_units)],
                    sd_send.at[i], sd_recv.at[i], at(z, x, t2),
                ).wait_recv()
            sd_own.wait()
            base[...] = own_hid[...].astype(f32) + jnp.dot(
                si[...], sdq[...], preferred_element_type=f32
            )

        pass_heads(1)
        lax.fori_loop(0, count, weigh, 0)
        for load in loads:
            load.wait()
        expert(0)
        pass_heads(2)
        expert(1)
        pass_heads(3)
        shared_inner()
        expert(3)
        expert(2)
        shared_out()

        cuts = [slice(start, start + 256) for start in range(0, quarter, 256)]

        def down_hop(b, c, down):
            return remote(
                passed.at[b, :, cuts[c]], arrived.at[down, b, :, cuts[c]],
                zr_send.at[b, c], zr_recv.at[down, b, c],
                at(z + (-1 if down else 1), x, t),
            )

        def owner_copy(c, i):
            _, t2 = mate(0, TP_FLIPS[i])
            rows = pl.ds(pl.multiple_of(t2 * rows_each, 16), rows_each)
            return remote(
                fin.at[rows, cuts[c]],
                out_ref.at[:, pl.ds(pl.multiple_of(t * quarter + 256 * c, 128), 256)],
                f_send.at[c, i], f_recv.at[c, i], at(z, x, t2),
            )

        def owner_own(c):
            rows = pl.ds(pl.multiple_of(t * rows_each, 16), rows_each)
            return pltpu.make_async_copy(
                fin.at[rows, cuts[c]],
                out_ref.at[:, pl.ds(pl.multiple_of(t * quarter + 256 * c, 128), 256)],
                f_recv.at[c, len(TP_FLIPS)],
            )

        def combine(k):
            b = nearest(k)
            for i in range(len(FLIPS)):
                x2, t2 = mate(*FLIPS[i])
                remote(
                    ret.at[0, :, columns(t2, quarter)], rr.at[b, x2 * tp_count + t2],
                    rt_send.at[b, i], rt_recv.at[b, i], at(z, x2, t2),
                ).wait_recv()
            back_own(b).wait()
            sel_t[...] = sel[b, :, 0:tokens].T
            for c, cut in enumerate(cuts):
                @pl.when((z >= b) & (z < planes - 1))
                def _():
                    down_hop(b, c, 1).wait_recv()

                @pl.when((z <= b) & (z > 0))
                def _():
                    down_hop(b, c, 0).wait_recv()

                total = jnp.dot(
                    sel_t[...], rr[b, :, :, cut].reshape(slots, 256), preferred_element_type=f32
                )
                total = total + arrived[1, b, :, cut].astype(f32)
                total = total + arrived[0, b, :, cut].astype(f32)
                if k:
                    passed[b, :, cut] = total.astype(bf16)

                    @pl.when(z > b)
                    def _():
                        down_hop(b, c, 1).start()

                    @pl.when(z < b)
                    def _():
                        down_hop(b, c, 0).start()
                else:
                    fin[:, cut] = (total + base[:, cut]).astype(bf16)
                    for i in range(len(TP_FLIPS)):
                        owner_copy(c, i).start()
                    owner_own(c).start()

        for k in range(planes - 1, -1, -1):
            combine(k)

        for c in range(len(cuts)):
            for i in range(len(TP_FLIPS)):
                _, t2 = mate(0, TP_FLIPS[i])
                remote(
                    fin.at[0:rows_each, cuts[c]],
                    out_ref.at[:, pl.ds(pl.multiple_of(t2 * quarter + 256 * c, 128), 256)],
                    f_send.at[c, i], f_recv.at[c, i], at(z, x, t2),
                ).wait_recv()
            owner_own(c).wait()

        for step in range(1, planes):
            along(step).wait_send()
        for k in range(planes):
            b = nearest(k)
            across(b).wait_send()
            for up in (1, 0):
                @pl.when(goes(b, up))
                def _():
                    z_hop(rblk, b, up, rz_send, rz_recv).wait_send()
                    z_hop(hblk, b, up, hz_send, hz_recv).wait_send()
            for i in range(len(FLIPS)):
                deal_copy(b, *resid_path[1:], i).wait_send()
                deal_copy(b, *heads_path[1:], i).wait_send()
                back_copy(b, 0, i).wait_send()
            if k:
                for c in range(len(cuts)):
                    down_hop(b, c, 0).wait_send()
        for i in range(len(TP_FLIPS)):
            sd_copies[i].wait_send()
            gather(i).wait_send()
            inner_copy(i).wait_send()
            for c in range(len(cuts)):
                owner_copy(c, i).wait_send()

    vmem = pl.BlockSpec(memory_space=pltpu.VMEM)
    anywhere = pl.BlockSpec(memory_space=pl.ANY)
    dma = pltpu.SemaphoreType.DMA
    flips, tps = len(FLIPS), len(TP_FLIPS)
    cut_count = quarter // 256
    return pl.pallas_call(
        kernel,
        out_shape=jax.ShapeDtypeStruct((rows_each, model), bf16),
        in_specs=[vmem] * 4 + [anywhere] * 8,
        out_specs=vmem,
        scratch_shapes=[
            pltpu.VMEM((count,) + packet.shape, bf16),
            pltpu.VMEM((1, span), f32),
            pltpu.VMEM((1, span), f32),
            pltpu.VMEM((HEAD_SIZE, span), f32),
            pltpu.VMEM((lanes, lanes), bf16),
            pltpu.VMEM((group, lanes), f32),
            pltpu.VMEM((count, capacity, 128), f32),
            pltpu.VMEM((planes, slots, lanes), bf16),
            pltpu.VMEM((tokens, slots), bf16),
            pltpu.VMEM((planes, tokens, quarter), bf16),
            pltpu.VMEM((planes, tokens, features), bf16),
            pltpu.VMEM((planes, slots, quarter), bf16),
            pltpu.VMEM((planes, slots, features), bf16),
            pltpu.VMEM((count, capacity, model), bf16),
            pltpu.VMEM((count, capacity, tp_count * features), bf16),
            pltpu.VMEM((pair, model), bf16),
            pltpu.VMEM((pair, model), bf16),
            pltpu.VMEM((count, capacity, model), bf16),
            pltpu.VMEM((planes, group, capacity, quarter), bf16),
            pltpu.VMEM((planes, tokens, quarter), bf16),
            pltpu.VMEM((2, planes, tokens, quarter), bf16),
            pltpu.VMEM((tokens, quarter), f32),
            pltpu.VMEM((tokens, quarter), bf16),
            pltpu.VMEM((tokens, tp_count * features), bf16),
            pltpu.VMEM((tokens, quarter), bf16),
            pltpu.VMEM((tokens, tp_count * shared_units), bf16),
            pltpu.VMEM((tp_count * shared_units, quarter), bf16),
            pltpu.VMEM(residual.shape, bf16),
            pltpu.VMEM(out_proj.shape, bf16),
            pltpu.VMEM(gate_w.shape, bf16),
            pltpu.VMEM(up_w.shape, bf16),
            pltpu.VMEM(down_w.shape, bf16),
            pltpu.VMEM(shared_gate.shape, bf16),
            pltpu.VMEM(shared_up.shape, bf16),
            dma((7,)),
            dma((2,)),
            dma((planes,)),
            dma((planes,)),
            dma((count,)),
            dma((2, planes)),
            dma((planes,)),
            dma((planes, flips)),
            dma((planes, flips + 1)),
            dma((2, planes)),
            dma((planes,)),
            dma((planes, flips)),
            dma((planes, flips + 1)),
            dma((tps,)),
            dma((tps + 1,)),
            dma((tps,)),
            dma((tps + 1,)),
            dma((tps,)),
            dma((tps,)),
            dma((planes, flips)),
            dma((planes, flips + 1)),
            dma((planes, cut_count)),
            dma((2, planes, cut_count)),
            dma((cut_count, tps)),
            dma((cut_count, tps + 1)),
        ],
        compiler_params=pltpu.CompilerParams(
            collective_id=call_id, has_side_effects=True, vmem_limit_bytes=63 * 1024 * 1024
        ),
        name="whole_layer",
    )(queries_t, packet, gain, ffn_gain, residual, *weights)


def scan_attention(query_rows, key_blocks, score_scale):
    start_state = (
        jnp.full((query_rows.shape[0],), -1e30, jnp.float32),
        jnp.zeros((query_rows.shape[0],), jnp.float32),
        jnp.zeros(query_rows.shape, jnp.float32),
    )

    def step(carry, key_slab):
        run_max, run_total, run_acc = carry
        scores = (
            lax.dot_general(
                query_rows,
                key_slab[:, :HEAD_SIZE],
                (((1,), (1,)), ((), ())),
                preferred_element_type=jnp.float32,
            )
            * score_scale
        )
        new_max = jnp.maximum(run_max, jnp.max(scores, axis=1))
        factor = jnp.exp(run_max - new_max)
        expo_terms = jnp.exp(scores - new_max[:, None])
        new_total = run_total * factor + jnp.sum(expo_terms, axis=1)
        new_acc = run_acc * factor[:, None] + jnp.dot(
            expo_terms.astype(jnp.bfloat16),
            key_slab[:, HEAD_SIZE:],
            preferred_element_type=jnp.float32,
        )
        return ((new_max, new_total, new_acc), None)

    (_, run_total, run_acc), _ = lax.scan(step, start_state, key_blocks)
    return run_acc / run_total[:, None]


def slot_ranks(member):
    order = jnp.arange(member.shape[0], dtype=jnp.int32)
    before = (order[:, None] > order[None, :]).astype(jnp.bfloat16)
    rank = jnp.dot(before, member.astype(jnp.bfloat16), preferred_element_type=jnp.float32)
    return jnp.where(member, rank.astype(jnp.int32), -1)


def expert_block(flat_rows, gate_local, up_local, down_local):
    gate_out = jnp.dot(flat_rows, gate_local, preferred_element_type=jnp.float32)
    up_out = jnp.dot(flat_rows, up_local, preferred_element_type=jnp.float32)
    expert_inner = (jax.nn.silu(gate_out) * up_out).astype(jnp.bfloat16)
    return jnp.dot(expert_inner, down_local, preferred_element_type=jnp.float32).astype(
        jnp.bfloat16
    )


def local(
    queries,
    key_matrix,
    values,
    query_gain,
    key_norm_gain,
    head_gain,
    out_proj,
    residual,
    ffn_gain,
    routes,
    route_weights,
    expert_gate,
    expert_up,
    expert_down,
    shared_gate,
    shared_up,
    shared_down,
):
    tok_count = queries.shape[0]
    head_count = queries.shape[1] // HEAD_SIZE
    sp_count = lax.axis_size("sp")
    tp_count = lax.axis_size("tp")
    tp_index = lax.axis_index("tp")
    sequence_total = tok_count * sp_count
    positions = lax.axis_index("sp") * tok_count + jnp.arange(tok_count, dtype=jnp.int32)
    cosine_table, sine_table = grid_tables(positions, sequence_total)
    rotated_query = apply_rotary(
        final_norm(
            queries.astype(jnp.float32).reshape(tok_count, head_count, HEAD_SIZE), query_gain
        ),
        cosine_table,
        sine_table,
    ).astype(jnp.bfloat16)
    rotated_key = (
        apply_rotary(
            final_norm(
                key_matrix.astype(jnp.float32).reshape(tok_count, 1, HEAD_SIZE), key_norm_gain
            ),
            cosine_table,
            sine_table,
        )
        .reshape(tok_count, HEAD_SIZE)
        .astype(jnp.bfloat16)
    )
    packed = jnp.concatenate([rotated_key, values], axis=1)
    score_scale = HEAD_SIZE ** (-0.5)
    topk_count = routes.shape[1]
    capacity = max(2, 2 * tok_count * topk_count // (sp_count * tp_count))
    lanes = 2 * HEAD_SIZE
    entries = tok_count * topk_count
    relayed = (
        tp_count == 4
        and sp_count == 2 * tp_count
        and capacity % 16 == 0
        and tok_count % (16 * tp_count) == 0
        and entries % lanes == 0
        and head_count * tok_count % 256 == 0
        and head_count % 2 == 0
    )
    if relayed:
        lane_total = -(-tok_count // 128) * 128
        scale_hi = lax.reduce_precision(route_weights, 8, 7)
        tables = jnp.concatenate(
            [routes.astype(jnp.float32), scale_hi, route_weights - scale_hi], axis=1
        ).T
        tables = jnp.pad(
            tables, ((0, -3 * topk_count % 16), (0, lane_total - tok_count)), constant_values=-1.0
        ).astype(jnp.bfloat16)
        tables = tables.reshape(tables.shape[0], -1, 128).transpose(1, 0, 2).reshape(-1, 128)
        scaled = rotated_query * jnp.asarray(score_scale, jnp.bfloat16)
        return whole_layer(
            scaled.transpose(2, 1, 0).reshape(HEAD_SIZE, head_count * tok_count),
            jnp.concatenate([packed, tables], axis=0),
            head_gain.reshape(head_count, HEAD_SIZE),
            ffn_gain.reshape(1, -1),
            residual,
            (out_proj, expert_gate[0], expert_up[0], expert_down[0], shared_gate, shared_up, shared_down),
            tok_count,
            capacity,
            topk_count,
            sp_count // tp_count,
            tp_count,
            0,
        )
    piece = exchange(packed, "sp", 0, True).reshape(sequence_total, lanes)
    query_rows = rotated_query.transpose(1, 0, 2).reshape(head_count * tok_count, HEAD_SIZE)
    block_length = key_block_rows(sequence_total)
    key_blocks = piece.reshape(sequence_total // block_length, block_length, lanes)
    attended = scan_attention(query_rows, key_blocks, score_scale)
    attended = attended.reshape(head_count, tok_count, HEAD_SIZE).transpose(1, 0, 2)
    head_out = final_norm(attended, head_gain.reshape(head_count, HEAD_SIZE))
    head_out = head_out.astype(jnp.bfloat16).reshape(tok_count, head_count * HEAD_SIZE)
    part_rows = tok_count // tp_count
    token_heads = exchange(
        head_out.reshape(tp_count, part_rows, head_count * HEAD_SIZE), "tp", 1, False
    )
    token_heads = token_heads.transpose(1, 0, 2).reshape(part_rows, -1)
    own_resid = lax.dynamic_slice_in_dim(residual, tp_index * part_rows, part_rows, 0)
    hidden_own = (
        own_resid.astype(jnp.float32)
        + jnp.dot(token_heads, out_proj, preferred_element_type=jnp.float32)
    ).astype(jnp.bfloat16)
    normed_own = final_norm(hidden_own.astype(jnp.float32), ffn_gain).astype(jnp.bfloat16)
    model_width = normed_own.shape[1]
    gate_local = expert_gate[0]
    up_local = expert_up[0]
    down_local = expert_down[0]
    normed = exchange(normed_own, "tp", 2, True).reshape(tok_count, model_width)
    slot_total = sp_count * capacity
    experts_here = jnp.arange(sp_count, dtype=jnp.int32) * tp_count + tp_index
    named = routes[:, :, None] == experts_here[None, None, :]
    member = jnp.any(named, axis=1)
    scale = jnp.sum(jnp.where(named, route_weights[:, :, None], 0.0), axis=1)
    rank = slot_ranks(member)
    slots = jnp.arange(capacity, dtype=jnp.int32)
    chosen = rank.T[:, None, :] == slots[None, :, None]
    select = chosen.astype(jnp.bfloat16).reshape(slot_total, tok_count)
    outgoing = jnp.dot(select, normed, preferred_element_type=jnp.float32).astype(jnp.bfloat16)
    arrived = exchange(outgoing.reshape(sp_count, capacity, model_width), "sp", 3, False)
    produced = expert_block(
        arrived.reshape(slot_total, model_width), gate_local, up_local, down_local
    )
    returned = exchange(produced.reshape(sp_count, capacity, model_width), "sp", 4, False).reshape(
        slot_total, model_width
    )
    combine = jnp.where(chosen, scale.T[:, None, :], 0.0).reshape(slot_total, tok_count)
    combine_hi = lax.reduce_precision(combine, 8, 7)
    combine_lo = (combine - combine_hi).astype(jnp.bfloat16)
    combine_hi = combine_hi.astype(jnp.bfloat16)

    def mix(weights):
        return lax.dot_general(
            weights, returned, (((0,), (0,)), ((), ())), preferred_element_type=jnp.float32
        )

    gate_part = jnp.dot(normed, shared_gate, preferred_element_type=jnp.float32)
    up_part = jnp.dot(normed, shared_up, preferred_element_type=jnp.float32)
    shared_inner = (jax.nn.silu(gate_part) * up_part).astype(jnp.bfloat16)
    shares = (
        jnp.dot(shared_inner, shared_down, preferred_element_type=jnp.float32)
        + mix(combine_hi)
        + mix(combine_lo)
    ).astype(jnp.bfloat16)
    shares = exchange(shares.reshape(tp_count, part_rows, model_width), "tp", 5, False)
    mixed_rows = jnp.sum(shares.astype(jnp.float32), axis=0)
    return (hidden_own.astype(jnp.float32) + mixed_rows).astype(jnp.bfloat16)


def solution(mesh):
    placed = (
        P("sp", "tp"),
        P("sp", "tp"),
        P("sp", "tp"),
        P(),
        P(),
        P("tp"),
        P(),
        P("sp", None),
        P(),
        P("sp", None),
        P("sp", None),
        P(("sp", "tp"), None, None),
        P(("sp", "tp"), None, None),
        P(("sp", "tp"), None, None),
        P(None, "tp"),
        P(None, "tp"),
        P("tp", None),
    )
    return jax.shard_map(
        local, mesh=mesh, in_specs=placed, out_specs=P(("sp", "tp"), None), check_vma=False
    )
```

```python
import jax
import jax.numpy as jnp
from jax import lax
from jax.experimental import pallas as pl
from jax.experimental.pallas import tpu as pltpu
from jax.sharding import PartitionSpec as P

HEAD_SIZE = 64
GRID_W = 64


EPS = 1e-06
THETA = 10000.0


def final_norm(field, gain):
    mean_sq = jnp.mean(field * field, axis=-1, keepdims=True)
    return field * lax.rsqrt(mean_sq + EPS) * gain


def grid_tables(positions, sequence_total):
    grid_rows = sequence_total // GRID_W
    row_pos = (positions // GRID_W - grid_rows // 2).astype(jnp.float32)
    col_pos = (positions % GRID_W - GRID_W // 2).astype(jnp.float32)
    quarter = HEAD_SIZE // 4
    inverse = THETA ** (-jnp.arange(quarter, dtype=jnp.float32) / quarter)
    angles = jnp.concatenate([row_pos[:, None] * inverse, col_pos[:, None] * inverse], axis=1)
    return (jnp.cos(angles), jnp.sin(angles))


def apply_rotary(field, cosine_table, sine_table):
    row_count, head_count = (field.shape[0], field.shape[1])
    quarter = HEAD_SIZE // 4
    pieces = field.reshape(row_count, head_count, 2, 2, quarter)
    front_half = pieces[:, :, :, 0, :].reshape(row_count, head_count, 2 * quarter)
    back_half = pieces[:, :, :, 1, :].reshape(row_count, head_count, 2 * quarter)
    cos_wide = cosine_table[:, None, :]
    sin_wide = sine_table[:, None, :]
    new_front = (front_half * cos_wide - back_half * sin_wide).reshape(
        row_count, head_count, 2, 1, quarter
    )
    new_back = (front_half * sin_wide + back_half * cos_wide).reshape(
        row_count, head_count, 2, 1, quarter
    )
    return jnp.concatenate([new_front, new_back], axis=3).reshape(row_count, head_count, HEAD_SIZE)


def exchange(block, axis, call_id, gather):
    count = lax.axis_size(axis)
    if count == 1:
        return block[None] if gather else block
    shape = (count,) + block.shape if gather else block.shape

    def kernel(in_ref, out_ref, send_sems, recv_sems, own_sem):
        me = lax.axis_index(axis)
        barrier = pltpu.get_barrier_semaphore()
        for step in range(1, count):
            pl.semaphore_signal(
                barrier,
                inc=1,
                device_id={axis: lax.rem(me + step, count)},
                device_id_type=pl.DeviceIdType.MESH,
            )
        own = pltpu.make_async_copy(in_ref if gather else in_ref.at[me], out_ref.at[me], own_sem)
        own.start()
        pl.semaphore_wait(barrier, count - 1)
        copies = []
        for step in range(1, count):
            peer = lax.rem(me + step, count)
            copy = pltpu.make_async_remote_copy(
                src_ref=in_ref if gather else in_ref.at[peer],
                dst_ref=out_ref.at[me],
                send_sem=send_sems.at[step],
                recv_sem=recv_sems.at[step],
                device_id={axis: peer},
                device_id_type=pl.DeviceIdType.MESH,
            )
            copy.start()
            copies.append(copy)
        own.wait()
        for copy in copies:
            copy.wait()

    return pl.pallas_call(
        kernel,
        out_shape=jax.ShapeDtypeStruct(shape, block.dtype),
        in_specs=[pl.BlockSpec(memory_space=pltpu.VMEM)],
        out_specs=pl.BlockSpec(memory_space=pltpu.VMEM),
        scratch_shapes=[
            pltpu.SemaphoreType.DMA((count,)),
            pltpu.SemaphoreType.DMA((count,)),
            pltpu.SemaphoreType.DMA,
        ],
        compiler_params=pltpu.CompilerParams(collective_id=call_id, has_side_effects=True),
        name="exchange_%d" % call_id,
    )(block)


def key_block_rows(piece_rows):
    return max((width for width in range(1, 2049) if piece_rows % width == 0))


MESH = pl.DeviceIdType.MESH
COLUMNS = 512
FLIPS = ((1, 2), (1, 3), (0, 2), (0, 3), (1, 0), (1, 1), (0, 1))
TP_FLIPS = (2, 3, 1)


def remote(source, target, send_sem, recv_sem, device):
    return pltpu.make_async_remote_copy(
        src_ref=source,
        dst_ref=target,
        send_sem=send_sem,
        recv_sem=recv_sem,
        device_id=device,
        device_id_type=MESH,
    )


def whole_layer(
    queries_t,
    own_kv,
    own_table,
    gain,
    ffn_gain,
    residual,
    weights,
    tokens,
    capacity,
    topk,
    width,
    tp_count,
    call_id,
):
    count = lax.axis_size("sp")
    planes = count // width
    group = width * tp_count
    span = queries_t.shape[1]
    heads = gain.shape[0]
    features = heads * HEAD_SIZE
    model = residual.shape[1]
    quarter = model // tp_count
    rows_each = tokens // tp_count
    chunk = 256
    lane_groups = -(-tokens // 128)
    lanes = 128 * lane_groups
    table_rows = own_table.shape[0]
    table_step = table_rows // lane_groups
    slots = group * capacity
    out_proj, gate_w, up_w, down_w, shared_gate, shared_up, shared_down = weights
    hidden_units = gate_w.shape[1]
    shared_units = shared_gate.shape[1]
    pair = width * capacity
    half = tokens // 2
    bf16, f32 = jnp.bfloat16, jnp.float32

    def kernel(
        q_ref, own_ref, tab_ref, gain_ref, ffn_ref, resid_ref, wo_hbm, wg_hbm, wu_hbm, wd_hbm,
        sg_hbm, su_hbm, sd_hbm, out_ref,
        kv, tabs, top, norm, acc, tri, ranks, scales, sel, sel_t, rblk, hblk, rpack, hpack,
        xr, xh, hs, ns, ret, rr, passed, arrived, base, fin, hg, own_hid, si, sdq,
        res, wo, wg, wu, wd, sg, su,
        w_sem, k_sem, tb_send, tb_recv, kz_send, kx_send, k_recv,
        rz_send, rz_recv, ri_send, ri_recv, hz_send, hz_recv, hi_send, hi_recv,
        hg_send, hg_recv, sd_send, sd_recv, si_send, si_recv,
        rt_send, rt_recv, zr_send, zr_recv, f_send, f_recv,
    ):
        me, t = lax.axis_index("sp"), lax.axis_index("tp")
        z, x = me // width, me % width
        p = x * tp_count + t
        side = z // 2
        inner = jnp.where((z == 1) | (z == 2), 1, 0)

        def nearest(k):
            near = k + inner * (1 - 2 * k) if k < 2 else k
            return near + side * (planes - 1 - 2 * near)

        def mate(dx, dt):
            x2 = 1 - x if dx else x
            t2 = t
            if dt & 2:
                t2 = t2 + 2 * (1 - 2 * (t // 2))
            if dt & 1:
                t2 = t2 + (1 - 2 * (t % 2))
            return x2, t2

        def at(plane, x2, t2):
            return {"sp": plane * width + x2, "tp": t2}

        arrived[...] = jnp.zeros(arrived.shape, bf16)
        barrier = pltpu.get_barrier_semaphore()
        for dx, dt in FLIPS:
            pl.semaphore_signal(barrier, inc=1, device_id=at(z, *mate(dx, dt)), device_id_type=MESH)
        for step in range(1, planes):
            for x2 in (x, 1 - x):
                pl.semaphore_signal(
                    barrier, inc=1, device_id=at(lax.rem(z + step, planes), x2, t),
                    device_id_type=MESH,
                )

        def columns(index, size):
            return pl.ds(pl.multiple_of(index * size, 128), size)

        locals_ = [
            pltpu.make_async_copy(resid_ref.at[:, columns(t, quarter)], rblk.at[z], k_sem.at[1]),
            pltpu.make_async_copy(own_ref, kv.at[me], k_sem.at[0]),
            pltpu.make_async_copy(tab_ref, tabs.at[me], k_sem.at[2]),
        ]
        for copy in locals_:
            copy.start()
        loads = [
            pltpu.make_async_copy(source, target, w_sem.at[i])
            for i, (source, target) in enumerate(
                [
                    (wo_hbm, wo), (wg_hbm, wg), (wu_hbm, wu), (wd_hbm, wd),
                    (sg_hbm, sg), (su_hbm, su), (resid_ref, res),
                ]
            )
        ]
        before = lax.broadcasted_iota(jnp.int32, (lanes, lanes), 0)
        after = lax.broadcasted_iota(jnp.int32, (lanes, lanes), 1)
        tri[...] = jnp.where(before < after, 1.0, 0.0).astype(bf16)
        for copy in locals_:
            copy.wait()
        pl.semaphore_wait(barrier, len(FLIPS) + 2 * (planes - 1))

        def along(k):
            return remote(
                own_ref, kv.at[me], kz_send.at[k], k_recv.at[me], at(nearest(k), x, t)
            )

        def table_copy(k, far):
            i = 2 * k + far
            return remote(
                tab_ref, tabs.at[me], tb_send.at[i], tb_recv.at[me],
                at(nearest(k), 1 - x if far else x, t),
            )

        def told(slot):
            return remote(tab_ref, tabs.at[slot], tb_send.at[1], tb_recv.at[slot], at(z, 1 - x, t))

        def came(slot):
            return remote(own_ref, kv.at[slot], kz_send.at[0], k_recv.at[slot], at(z, 1 - x, t))

        def across(plane):
            slot = plane * width + x
            return remote(kv.at[slot], kv.at[slot], kx_send.at[plane], k_recv.at[slot], at(z, 1 - x, t))

        def z_hop(blk, b, up, ssem, rsem):
            return remote(
                blk.at[b], blk.at[b], ssem.at[up, b], rsem.at[b],
                at(z + (1 if up else -1), x, t),
            )

        def goes(b, up):
            return (b <= z) & (z < planes - 1) if up else (b >= z) & (z > 0)

        def forward(blk, b, ssem, rsem):
            for up in (1, 0):
                @pl.when(goes(b, up))
                def _():
                    z_hop(blk, b, up, ssem, rsem).start()

        def landed(b, wide, dst, x2, t2):
            return dst.at[b * width + x2, :, columns(t2, wide)]

        def deal_copy(b, pack, dst, wide, ssem, rsem, i):
            x2, t2 = mate(*FLIPS[i])
            rows = pl.ds(pl.multiple_of((x2 * tp_count + t2) * capacity, 16), capacity)
            return remote(
                pack.at[b, rows], landed(b, wide, dst, x, t), ssem.at[b, i], rsem.at[b, i],
                at(z, x2, t2),
            )

        def deal_own(b, pack, dst, wide, rsem):
            rows = pl.ds(pl.multiple_of(p * capacity, 16), capacity)
            return pltpu.make_async_copy(
                pack.at[b, rows], landed(b, wide, dst, x, t), rsem.at[b, len(FLIPS)]
            )

        def deal(b, blk, pack, dst, wide, ssem, rsem):
            for start in range(0, slots, tokens):
                pack[b, start : start + tokens, :] = jnp.dot(
                    sel[b, start : start + tokens, 0:tokens], blk[b], preferred_element_type=f32
                ).astype(bf16)
            for i in range(len(FLIPS)):
                deal_copy(b, pack, dst, wide, ssem, rsem, i).start()
            deal_own(b, pack, dst, wide, rsem).start()

        def dealt(b, pack, dst, wide, ssem, rsem):
            for i in range(len(FLIPS)):
                x2, t2 = mate(*FLIPS[i])
                remote(
                    pack.at[b, 0:capacity], landed(b, wide, dst, x2, t2), ssem.at[b, i],
                    rsem.at[b, i], at(z, x2, t2),
                ).wait_recv()
            deal_own(b, pack, dst, wide, rsem).wait()

        resid_path = (rblk, rpack, xr, quarter, ri_send, ri_recv)
        heads_path = (hblk, hpack, xh, features, hi_send, hi_recv)

        def table(slot):
            return tabs[slot].astype(f32)

        def index(b):
            rows = table(b * width + x)
            named = (lax.broadcasted_iota(jnp.int32, (group, 128), 0) + z * group).astype(f32)
            for j in range(lane_groups):
                hit = jnp.zeros((group, 128), f32)
                for k in range(topk):
                    row = rows[j * table_step + k : j * table_step + k + 1]
                    hit = jnp.where(row == named, 1.0, hit)
                ranks[0:group, 128 * j : 128 * j + 128] = hit
            member = ranks[0:group, :]
            rank = jnp.dot(member.astype(bf16), tri[...], preferred_element_type=f32)
            ranks[0:group, :] = jnp.where(member > 0.5, rank, -1.0)
            wanted = lax.broadcasted_iota(jnp.int32, (capacity, 128), 0).astype(f32)
            for e in range(group):
                for j in range(lane_groups):
                    row = ranks[e : e + 1, 128 * j : 128 * j + 128]
                    sel[b, e * capacity : (e + 1) * capacity, 128 * j : 128 * j + 128] = jnp.where(
                        row == wanted, 1.0, 0.0
                    ).astype(bf16)

        def weigh(slot, carry):
            rows = table(slot)
            mine_is = (z * group + p).astype(f32)
            amounts = []
            for j in range(lane_groups):
                hit = jnp.zeros((1, 128), f32)
                amount = jnp.zeros((1, 128), f32)
                for k in range(topk):
                    at_row = j * table_step + k
                    same = rows[at_row : at_row + 1] == mine_is
                    high = rows[at_row + topk : at_row + topk + 1]
                    low = rows[at_row + 2 * topk : at_row + 2 * topk + 1]
                    hit = jnp.where(same, 1.0, hit)
                    amount = jnp.where(same, high + low, amount)
                ranks[0:8, 128 * j : 128 * j + 128] = jnp.broadcast_to(hit, (8, 128))
                amounts.append(amount)
            member = ranks[0:8, :]
            rank = jnp.dot(member.astype(bf16), tri[...], preferred_element_type=f32)
            ranks[0:8, :] = jnp.where(member > 0.5, rank, -1.0)
            wanted = lax.broadcasted_iota(jnp.int32, (capacity, 128), 0).astype(f32)
            summed = jnp.zeros((capacity, 128), f32)
            for j in range(lane_groups):
                row = ranks[0:1, 128 * j : 128 * j + 128]
                summed = summed + jnp.where(row == wanted, amounts[j], 0.0)
            scales[slot] = jnp.broadcast_to(
                jnp.sum(summed, axis=1, keepdims=True), (capacity, 128)
            )
            return carry

        def absorb(slot):
            keys = kv[slot, 0:tokens, 0:HEAD_SIZE]
            vals_t = kv[slot, 0:tokens, HEAD_SIZE : 2 * HEAD_SIZE].T
            for start in range(0, span, chunk):
                part = pl.ds(start, chunk)
                scores = jnp.dot(keys, q_ref[:, part], preferred_element_type=f32)
                old = top[:, part]
                peak = jnp.maximum(old, jnp.max(scores, axis=0, keepdims=True))
                factor = jnp.exp(old - peak)
                terms = jnp.exp(scores - peak)
                norm[:, part] = norm[:, part] * factor + jnp.sum(terms, axis=0, keepdims=True)
                acc[:, part] = acc[:, part] * factor + jnp.dot(
                    vals_t, terms.astype(bf16), preferred_element_type=f32
                )
                top[:, part] = peak

        def each_side(step, body):
            def side_of(i, carry):
                b = z + (2 * i - 1) * step

                @pl.when((b >= 0) & (b < planes))
                def _():
                    body(b)

                return carry

            lax.fori_loop(0, 2, side_of, 0)

        def pass_resid(step):
            def body(b):
                z_hop(rblk, b, 0, rz_send, rz_recv).wait_recv()
                forward(rblk, b, rz_send, rz_recv)
                told(b * width + x).wait_recv()
                index(b)
                deal(b, *resid_path)

            each_side(step, body)

        def pass_heads(step):
            def body(b):
                z_hop(hblk, b, 0, hz_send, hz_recv).wait_recv()
                forward(hblk, b, hz_send, hz_recv)
                deal(b, *heads_path)

            each_side(step, body)

        for k in range(1, planes):
            table_copy(k, 0).start()
        for k in range(1, planes):
            along(k).start()
        across(z).start()
        forward(rblk, z, rz_send, rz_recv)
        for k in range(planes):
            table_copy(k, 1).start()
        index(z)
        deal(z, *resid_path)
        for load in loads:
            load.start()
        sd_copies = []
        for i, dt in enumerate(TP_FLIPS):
            _, t2 = mate(0, dt)
            copy = remote(
                sd_hbm.at[:, columns(t2, quarter)],
                sdq.at[pl.ds(pl.multiple_of(t * shared_units, 16), shared_units)],
                sd_send.at[i], sd_recv.at[i], at(z, x, t2),
            )
            copy.start()
            sd_copies.append(copy)
        sd_own = pltpu.make_async_copy(
            sd_hbm.at[:, columns(t, quarter)],
            sdq.at[pl.ds(pl.multiple_of(t * shared_units, 16), shared_units)],
            sd_recv.at[len(TP_FLIPS)],
        )
        sd_own.start()
        top[...] = jnp.full(top.shape, -1e30, f32)
        norm[...] = jnp.zeros(norm.shape, f32)
        acc[...] = jnp.zeros(acc.shape, f32)
        absorb(me)

        def attend(k, far):
            slot = nearest(k) * width + ((1 - x) if far else x)
            came(slot).wait_recv()
            if not far:
                across(nearest(k)).start()
            absorb(slot)

        for k in range(1, planes):
            attend(k, False)
        attend(0, True)
        attend(1, True)
        pass_resid(1)
        attend(2, True)
        attend(3, True)

        attended = acc[...] / norm[...]
        mean_sq = jnp.mean(attended * attended, axis=0, keepdims=True)
        rows = (attended * lax.rsqrt(mean_sq + EPS)).T
        for h in range(heads):
            hblk[z, :, h * HEAD_SIZE : (h + 1) * HEAD_SIZE] = (
                rows[h * tokens : (h + 1) * tokens] * gain_ref[h : h + 1, :]
            ).astype(bf16)

        forward(hblk, z, hz_send, hz_recv)
        deal(z, *heads_path)

        def gather(i):
            _, t2 = mate(0, TP_FLIPS[i])
            if i == 1:
                _, t3 = mate(0, 2)
                _, t2 = mate(0, 1)
                rows = hg.at[:, columns(t3, features)]
                return remote(rows, rows, hg_send.at[i], hg_recv.at[i], at(z, x, t2))
            return remote(
                hblk.at[z], hg.at[:, columns(t, features)], hg_send.at[i], hg_recv.at[i],
                at(z, x, t2),
            )

        hg_own = pltpu.make_async_copy(
            hblk.at[z], hg.at[:, columns(t, features)], hg_recv.at[len(TP_FLIPS)]
        )
        hg_own.start()

        def normalize(head_rows, resid_at):
            count_rows = head_rows.shape[0]
            squares = jnp.zeros((count_rows, 1), f32)
            for start in range(0, model, COLUMNS):
                part = slice(start, start + COLUMNS)
                field = jnp.dot(head_rows, wo[:, part], preferred_element_type=f32)
                field = (resid_at(part).astype(f32) + field).astype(bf16)
                hs[:, part] = field
                field = field.astype(f32)
                squares = squares + jnp.sum(field * field, axis=1, keepdims=True)
            inverse = lax.rsqrt(squares / model + EPS)
            for start in range(0, model, COLUMNS):
                part = slice(start, start + COLUMNS)
                ns[:, part] = (hs[:, part].astype(f32) * inverse * ffn_ref[:, part]).astype(bf16)

        def glu(gate_ref, up_ref):
            gate = jnp.dot(ns[...], gate_ref[...], preferred_element_type=f32)
            up = jnp.dot(ns[...], up_ref[...], preferred_element_type=f32)
            return (gate / (1.0 + jnp.exp(-gate)) * up).astype(bf16)

        def back_copy(b, j, i):
            x2, t2 = mate(*FLIPS[i])
            return remote(
                ret.at[b * width + x2, :, columns(t2, quarter)], rr.at[b, p],
                rt_send.at[b, i], rt_recv.at[b, i], at(z, x2, t2),
            )

        def back_own(b):
            return pltpu.make_async_copy(
                ret.at[b * width + x, :, columns(t, quarter)], rr.at[b, p],
                rt_recv.at[b, len(FLIPS)],
            )

        def expert(k):
            b = nearest(k)
            dealt(b, *resid_path[1:])
            dealt(b, *heads_path[1:])
            both = pl.ds(b * width, width)

            def resid_at(part):
                return xr[both, :, part].reshape(pair, COLUMNS)

            normalize(xh[both].reshape(pair, tp_count * features), resid_at)
            inner_rows = glu(wg, wu)
            scale = scales[both].reshape(pair, 128)[:, 0:1]
            for start in range(0, model, COLUMNS):
                part = slice(start, start + COLUMNS)
                made = jnp.dot(inner_rows, wd[:, part], preferred_element_type=f32) * scale
                ret[both, :, part] = made.astype(bf16).reshape(width, capacity, COLUMNS)

        def give_back(k):
            b = nearest(k)
            for i in range(len(FLIPS)):
                back_copy(b, 0, i).start()
            back_own(b).start()

        def inner_copy(i):
            _, t2 = mate(0, TP_FLIPS[i])
            return remote(
                si.at[:, columns(t, shared_units)], si.at[:, columns(t, shared_units)],
                si_send.at[i], si_recv.at[i], at(z, x, t2),
            )

        def shared_inner():
            for i in range(len(TP_FLIPS)):
                _, t2 = mate(0, TP_FLIPS[i])
                remote(
                    hblk.at[z], hg.at[:, columns(t2, features)], hg_send.at[i], hg_recv.at[i],
                    at(z, x, t2),
                ).wait_recv()
                if i == 0:
                    gather(1).start()
            hg_own.wait()
            for start in (0, half):
                span_rows = slice(start, start + half)
                normalize(hg[span_rows, :], lambda part: res[span_rows, part])
                own_hid[span_rows, :] = hs[:, columns(t, quarter)]
                si[span_rows, columns(t, shared_units)] = glu(sg, su)
            for i in range(len(TP_FLIPS)):
                inner_copy(i).start()

        def shared_out():
            for i in range(len(TP_FLIPS)):
                _, t2 = mate(0, TP_FLIPS[i])
                remote(
                    si.at[:, columns(t, shared_units)], si.at[:, columns(t2, shared_units)],
                    si_send.at[i], si_recv.at[i], at(z, x, t2),
                ).wait_recv()
                remote(
                    sd_hbm.at[:, columns(t2, quarter)],
                    sdq.at[pl.ds(pl.multiple_of(t2 * shared_units, 16), shared_units)],
                    sd_send.at[i], sd_recv.at[i], at(z, x, t2),
                ).wait_recv()
            sd_own.wait()
            base[...] = own_hid[...].astype(f32) + jnp.dot(
                si[...], sdq[...], preferred_element_type=f32
            )

        pass_resid(2)
        pass_heads(1)
        for i in (0, 2):
            gather(i).start()
        pass_resid(3)
        pass_heads(2)
        pass_heads(3)
        for step in range(planes):
            told(step * width + (1 - x)).wait_recv()
        lax.fori_loop(0, count, weigh, 0)
        for load in loads:
            load.wait()
        expert(0)
        expert(1)
        shared_inner()
        give_back(1)
        expert(3)
        give_back(3)
        expert(2)
        give_back(2)
        give_back(0)

        cuts = [slice(start, start + 256) for start in range(0, quarter, 256)]

        def down_hop(b, c, down):
            return remote(
                passed.at[b, :, cuts[c]], arrived.at[down, b, :, cuts[c]],
                zr_send.at[b, c], zr_recv.at[down, b, c],
                at(z + (-1 if down else 1), x, t),
            )

        def owner_copy(c, i):
            _, t2 = mate(0, TP_FLIPS[i])
            rows = pl.ds(pl.multiple_of(t2 * rows_each, 16), rows_each)
            return remote(
                fin.at[rows, cuts[c]],
                out_ref.at[:, pl.ds(pl.multiple_of(t * quarter + 256 * c, 128), 256)],
                f_send.at[c, i], f_recv.at[c, i], at(z, x, t2),
            )

        def owner_own(c):
            rows = pl.ds(pl.multiple_of(t * rows_each, 16), rows_each)
            return pltpu.make_async_copy(
                fin.at[rows, cuts[c]],
                out_ref.at[:, pl.ds(pl.multiple_of(t * quarter + 256 * c, 128), 256)],
                f_recv.at[c, len(TP_FLIPS)],
            )

        def combine(k):
            b = nearest(k)
            for i in range(len(FLIPS)):
                x2, t2 = mate(*FLIPS[i])
                remote(
                    ret.at[0, :, columns(t2, quarter)], rr.at[b, x2 * tp_count + t2],
                    rt_send.at[b, i], rt_recv.at[b, i], at(z, x2, t2),
                ).wait_recv()
            back_own(b).wait()
            sel_t[...] = sel[b, :, 0:tokens].T
            for c, cut in enumerate(cuts):
                @pl.when((z >= b) & (z < planes - 1))
                def _():
                    down_hop(b, c, 1).wait_recv()

                @pl.when((z <= b) & (z > 0))
                def _():
                    down_hop(b, c, 0).wait_recv()

                total = jnp.dot(
                    sel_t[...], rr[b, :, :, cut].reshape(slots, 256), preferred_element_type=f32
                )
                total = total + arrived[1, b, :, cut].astype(f32)
                total = total + arrived[0, b, :, cut].astype(f32)
                if k:
                    passed[b, :, cut] = total.astype(bf16)

                    @pl.when(z > b)
                    def _():
                        down_hop(b, c, 1).start()

                    @pl.when(z < b)
                    def _():
                        down_hop(b, c, 0).start()
                else:
                    fin[:, cut] = (total + base[:, cut]).astype(bf16)
                    for i in range(len(TP_FLIPS)):
                        owner_copy(c, i).start()
                    owner_own(c).start()

        for k in range(planes - 1, 0, -1):
            combine(k)
        shared_out()
        combine(0)

        for c in range(len(cuts)):
            for i in range(len(TP_FLIPS)):
                _, t2 = mate(0, TP_FLIPS[i])
                remote(
                    fin.at[0:rows_each, cuts[c]],
                    out_ref.at[:, pl.ds(pl.multiple_of(t2 * quarter + 256 * c, 128), 256)],
                    f_send.at[c, i], f_recv.at[c, i], at(z, x, t2),
                ).wait_recv()
            owner_own(c).wait()

        for step in range(1, planes):
            along(step).wait_send()
            table_copy(step, 0).wait_send()
        for k in range(planes):
            b = nearest(k)
            across(b).wait_send()
            table_copy(k, 1).wait_send()
            for up in (1, 0):
                @pl.when(goes(b, up))
                def _():
                    z_hop(rblk, b, up, rz_send, rz_recv).wait_send()
                    z_hop(hblk, b, up, hz_send, hz_recv).wait_send()
            for i in range(len(FLIPS)):
                deal_copy(b, *resid_path[1:], i).wait_send()
                deal_copy(b, *heads_path[1:], i).wait_send()
                back_copy(b, 0, i).wait_send()
            if k:
                for c in range(len(cuts)):
                    down_hop(b, c, 0).wait_send()
        for i in range(len(TP_FLIPS)):
            sd_copies[i].wait_send()
            gather(i).wait_send()
            inner_copy(i).wait_send()
            for c in range(len(cuts)):
                owner_copy(c, i).wait_send()

    vmem = pl.BlockSpec(memory_space=pltpu.VMEM)
    anywhere = pl.BlockSpec(memory_space=pl.ANY)
    dma = pltpu.SemaphoreType.DMA
    flips, tps = len(FLIPS), len(TP_FLIPS)
    cut_count = quarter // 256
    return pl.pallas_call(
        kernel,
        out_shape=jax.ShapeDtypeStruct((rows_each, model), bf16),
        in_specs=[vmem] * 5 + [anywhere] * 8,
        out_specs=vmem,
        scratch_shapes=[
            pltpu.VMEM((count,) + own_kv.shape, bf16),
            pltpu.VMEM((count,) + own_table.shape, bf16),
            pltpu.VMEM((1, span), f32),
            pltpu.VMEM((1, span), f32),
            pltpu.VMEM((HEAD_SIZE, span), f32),
            pltpu.VMEM((lanes, lanes), bf16),
            pltpu.VMEM((group, lanes), f32),
            pltpu.VMEM((count, capacity, 128), f32),
            pltpu.VMEM((planes, slots, lanes), bf16),
            pltpu.VMEM((tokens, slots), bf16),
            pltpu.VMEM((planes, tokens, quarter), bf16),
            pltpu.VMEM((planes, tokens, features), bf16),
            pltpu.VMEM((planes, slots, quarter), bf16),
            pltpu.VMEM((planes, slots, features), bf16),
            pltpu.VMEM((count, capacity, model), bf16),
            pltpu.VMEM((count, capacity, tp_count * features), bf16),
            pltpu.VMEM((pair, model), bf16),
            pltpu.VMEM((pair, model), bf16),
            pltpu.VMEM((count, capacity, model), bf16),
            pltpu.VMEM((planes, group, capacity, quarter), bf16),
            pltpu.VMEM((planes, tokens, quarter), bf16),
            pltpu.VMEM((2, planes, tokens, quarter), bf16),
            pltpu.VMEM((tokens, quarter), f32),
            pltpu.VMEM((tokens, quarter), bf16),
            pltpu.VMEM((tokens, tp_count * features), bf16),
            pltpu.VMEM((tokens, quarter), bf16),
            pltpu.VMEM((tokens, tp_count * shared_units), bf16),
            pltpu.VMEM((tp_count * shared_units, quarter), bf16),
            pltpu.VMEM(residual.shape, bf16),
            pltpu.VMEM(out_proj.shape, bf16),
            pltpu.VMEM(gate_w.shape, bf16),
            pltpu.VMEM(up_w.shape, bf16),
            pltpu.VMEM(down_w.shape, bf16),
            pltpu.VMEM(shared_gate.shape, bf16),
            pltpu.VMEM(shared_up.shape, bf16),
            dma((7,)),
            dma((3,)),
            dma((2 * planes,)),
            dma((count,)),
            dma((planes,)),
            dma((planes,)),
            dma((count,)),
            dma((2, planes)),
            dma((planes,)),
            dma((planes, flips)),
            dma((planes, flips + 1)),
            dma((2, planes)),
            dma((planes,)),
            dma((planes, flips)),
            dma((planes, flips + 1)),
            dma((tps,)),
            dma((tps + 1,)),
            dma((tps,)),
            dma((tps + 1,)),
            dma((tps,)),
            dma((tps,)),
            dma((planes, flips)),
            dma((planes, flips + 1)),
            dma((planes, cut_count)),
            dma((2, planes, cut_count)),
            dma((cut_count, tps)),
            dma((cut_count, tps + 1)),
        ],
        compiler_params=pltpu.CompilerParams(
            collective_id=call_id, has_side_effects=True, vmem_limit_bytes=63 * 1024 * 1024
        ),
        name="whole_layer",
    )(queries_t, own_kv, own_table, gain, ffn_gain, residual, *weights)


def scan_attention(query_rows, key_blocks, score_scale):
    start_state = (
        jnp.full((query_rows.shape[0],), -1e30, jnp.float32),
        jnp.zeros((query_rows.shape[0],), jnp.float32),
        jnp.zeros(query_rows.shape, jnp.float32),
    )

    def step(carry, key_slab):
        run_max, run_total, run_acc = carry
        scores = (
            lax.dot_general(
                query_rows,
                key_slab[:, :HEAD_SIZE],
                (((1,), (1,)), ((), ())),
                preferred_element_type=jnp.float32,
            )
            * score_scale
        )
        new_max = jnp.maximum(run_max, jnp.max(scores, axis=1))
        factor = jnp.exp(run_max - new_max)
        expo_terms = jnp.exp(scores - new_max[:, None])
        new_total = run_total * factor + jnp.sum(expo_terms, axis=1)
        new_acc = run_acc * factor[:, None] + jnp.dot(
            expo_terms.astype(jnp.bfloat16),
            key_slab[:, HEAD_SIZE:],
            preferred_element_type=jnp.float32,
        )
        return ((new_max, new_total, new_acc), None)

    (_, run_total, run_acc), _ = lax.scan(step, start_state, key_blocks)
    return run_acc / run_total[:, None]


def slot_ranks(member):
    order = jnp.arange(member.shape[0], dtype=jnp.int32)
    before = (order[:, None] > order[None, :]).astype(jnp.bfloat16)
    rank = jnp.dot(before, member.astype(jnp.bfloat16), preferred_element_type=jnp.float32)
    return jnp.where(member, rank.astype(jnp.int32), -1)


def expert_block(flat_rows, gate_local, up_local, down_local):
    gate_out = jnp.dot(flat_rows, gate_local, preferred_element_type=jnp.float32)
    up_out = jnp.dot(flat_rows, up_local, preferred_element_type=jnp.float32)
    expert_inner = (jax.nn.silu(gate_out) * up_out).astype(jnp.bfloat16)
    return jnp.dot(expert_inner, down_local, preferred_element_type=jnp.float32).astype(
        jnp.bfloat16
    )


def local(
    queries,
    key_matrix,
    values,
    query_gain,
    key_norm_gain,
    head_gain,
    out_proj,
    residual,
    ffn_gain,
    routes,
    route_weights,
    expert_gate,
    expert_up,
    expert_down,
    shared_gate,
    shared_up,
    shared_down,
):
    tok_count = queries.shape[0]
    head_count = queries.shape[1] // HEAD_SIZE
    sp_count = lax.axis_size("sp")
    tp_count = lax.axis_size("tp")
    tp_index = lax.axis_index("tp")
    sequence_total = tok_count * sp_count
    positions = lax.axis_index("sp") * tok_count + jnp.arange(tok_count, dtype=jnp.int32)
    cosine_table, sine_table = grid_tables(positions, sequence_total)
    rotated_query = apply_rotary(
        final_norm(
            queries.astype(jnp.float32).reshape(tok_count, head_count, HEAD_SIZE), query_gain
        ),
        cosine_table,
        sine_table,
    ).astype(jnp.bfloat16)
    rotated_key = (
        apply_rotary(
            final_norm(
                key_matrix.astype(jnp.float32).reshape(tok_count, 1, HEAD_SIZE), key_norm_gain
            ),
            cosine_table,
            sine_table,
        )
        .reshape(tok_count, HEAD_SIZE)
        .astype(jnp.bfloat16)
    )
    packed = jnp.concatenate([rotated_key, values], axis=1)
    score_scale = HEAD_SIZE ** (-0.5)
    topk_count = routes.shape[1]
    capacity = max(2, 2 * tok_count * topk_count // (sp_count * tp_count))
    lanes = 2 * HEAD_SIZE
    entries = tok_count * topk_count
    relayed = (
        tp_count == 4
        and sp_count == 2 * tp_count
        and capacity % 16 == 0
        and tok_count % (16 * tp_count) == 0
        and entries % lanes == 0
        and head_count * tok_count % 256 == 0
        and head_count % 2 == 0
    )
    if relayed:
        lane_total = -(-tok_count // 128) * 128
        scale_hi = lax.reduce_precision(route_weights, 8, 7)
        tables = jnp.concatenate(
            [routes.astype(jnp.float32), scale_hi, route_weights - scale_hi], axis=1
        ).T
        tables = jnp.pad(
            tables, ((0, -3 * topk_count % 16), (0, lane_total - tok_count)), constant_values=-1.0
        ).astype(jnp.bfloat16)
        tables = tables.reshape(tables.shape[0], -1, 128).transpose(1, 0, 2).reshape(-1, 128)
        scaled = rotated_query * jnp.asarray(score_scale, jnp.bfloat16)
        return whole_layer(
            scaled.transpose(2, 1, 0).reshape(HEAD_SIZE, head_count * tok_count),
            packed,
            tables,
            head_gain.reshape(head_count, HEAD_SIZE),
            ffn_gain.reshape(1, -1),
            residual,
            (out_proj, expert_gate[0], expert_up[0], expert_down[0], shared_gate, shared_up, shared_down),
            tok_count,
            capacity,
            topk_count,
            sp_count // tp_count,
            tp_count,
            0,
        )
    piece = exchange(packed, "sp", 0, True).reshape(sequence_total, lanes)
    query_rows = rotated_query.transpose(1, 0, 2).reshape(head_count * tok_count, HEAD_SIZE)
    block_length = key_block_rows(sequence_total)
    key_blocks = piece.reshape(sequence_total // block_length, block_length, lanes)
    attended = scan_attention(query_rows, key_blocks, score_scale)
    attended = attended.reshape(head_count, tok_count, HEAD_SIZE).transpose(1, 0, 2)
    head_out = final_norm(attended, head_gain.reshape(head_count, HEAD_SIZE))
    head_out = head_out.astype(jnp.bfloat16).reshape(tok_count, head_count * HEAD_SIZE)
    part_rows = tok_count // tp_count
    token_heads = exchange(
        head_out.reshape(tp_count, part_rows, head_count * HEAD_SIZE), "tp", 1, False
    )
    token_heads = token_heads.transpose(1, 0, 2).reshape(part_rows, -1)
    own_resid = lax.dynamic_slice_in_dim(residual, tp_index * part_rows, part_rows, 0)
    hidden_own = (
        own_resid.astype(jnp.float32)
        + jnp.dot(token_heads, out_proj, preferred_element_type=jnp.float32)
    ).astype(jnp.bfloat16)
    normed_own = final_norm(hidden_own.astype(jnp.float32), ffn_gain).astype(jnp.bfloat16)
    model_width = normed_own.shape[1]
    gate_local = expert_gate[0]
    up_local = expert_up[0]
    down_local = expert_down[0]
    normed = exchange(normed_own, "tp", 2, True).reshape(tok_count, model_width)
    slot_total = sp_count * capacity
    experts_here = jnp.arange(sp_count, dtype=jnp.int32) * tp_count + tp_index
    named = routes[:, :, None] == experts_here[None, None, :]
    member = jnp.any(named, axis=1)
    scale = jnp.sum(jnp.where(named, route_weights[:, :, None], 0.0), axis=1)
    rank = slot_ranks(member)
    slots = jnp.arange(capacity, dtype=jnp.int32)
    chosen = rank.T[:, None, :] == slots[None, :, None]
    select = chosen.astype(jnp.bfloat16).reshape(slot_total, tok_count)
    outgoing = jnp.dot(select, normed, preferred_element_type=jnp.float32).astype(jnp.bfloat16)
    arrived = exchange(outgoing.reshape(sp_count, capacity, model_width), "sp", 3, False)
    produced = expert_block(
        arrived.reshape(slot_total, model_width), gate_local, up_local, down_local
    )
    returned = exchange(produced.reshape(sp_count, capacity, model_width), "sp", 4, False).reshape(
        slot_total, model_width
    )
    combine = jnp.where(chosen, scale.T[:, None, :], 0.0).reshape(slot_total, tok_count)
    combine_hi = lax.reduce_precision(combine, 8, 7)
    combine_lo = (combine - combine_hi).astype(jnp.bfloat16)
    combine_hi = combine_hi.astype(jnp.bfloat16)

    def mix(weights):
        return lax.dot_general(
            weights, returned, (((0,), (0,)), ((), ())), preferred_element_type=jnp.float32
        )

    gate_part = jnp.dot(normed, shared_gate, preferred_element_type=jnp.float32)
    up_part = jnp.dot(normed, shared_up, preferred_element_type=jnp.float32)
    shared_inner = (jax.nn.silu(gate_part) * up_part).astype(jnp.bfloat16)
    shares = (
        jnp.dot(shared_inner, shared_down, preferred_element_type=jnp.float32)
        + mix(combine_hi)
        + mix(combine_lo)
    ).astype(jnp.bfloat16)
    shares = exchange(shares.reshape(tp_count, part_rows, model_width), "tp", 5, False)
    mixed_rows = jnp.sum(shares.astype(jnp.float32), axis=0)
    return (hidden_own.astype(jnp.float32) + mixed_rows).astype(jnp.bfloat16)


def solution(mesh):
    placed = (
        P("sp", "tp"),
        P("sp", "tp"),
        P("sp", "tp"),
        P(),
        P(),
        P("tp"),
        P(),
        P("sp", None),
        P(),
        P("sp", None),
        P("sp", None),
        P(("sp", "tp"), None, None),
        P(("sp", "tp"), None, None),
        P(("sp", "tp"), None, None),
        P(None, "tp"),
        P(None, "tp"),
        P("tp", None),
    )
    return jax.shard_map(
        local, mesh=mesh, in_specs=placed, out_specs=P(("sp", "tp"), None), check_vma=False
    )
```

```python
import jax
import jax.numpy as jnp
from jax import lax
from jax.experimental import pallas as pl
from jax.experimental.pallas import tpu as pltpu
from jax.sharding import PartitionSpec as P

HEAD_SIZE = 64
GRID_W = 64


EPS = 1e-06
THETA = 10000.0


def final_norm(field, gain):
    mean_sq = jnp.mean(field * field, axis=-1, keepdims=True)
    return field * lax.rsqrt(mean_sq + EPS) * gain


def grid_tables(positions, sequence_total):
    grid_rows = sequence_total // GRID_W
    row_pos = (positions // GRID_W - grid_rows // 2).astype(jnp.float32)
    col_pos = (positions % GRID_W - GRID_W // 2).astype(jnp.float32)
    quarter = HEAD_SIZE // 4
    inverse = THETA ** (-jnp.arange(quarter, dtype=jnp.float32) / quarter)
    angles = jnp.concatenate([row_pos[:, None] * inverse, col_pos[:, None] * inverse], axis=1)
    return (jnp.cos(angles), jnp.sin(angles))


def apply_rotary(field, cosine_table, sine_table):
    row_count, head_count = (field.shape[0], field.shape[1])
    quarter = HEAD_SIZE // 4
    pieces = field.reshape(row_count, head_count, 2, 2, quarter)
    front_half = pieces[:, :, :, 0, :].reshape(row_count, head_count, 2 * quarter)
    back_half = pieces[:, :, :, 1, :].reshape(row_count, head_count, 2 * quarter)
    cos_wide = cosine_table[:, None, :]
    sin_wide = sine_table[:, None, :]
    new_front = (front_half * cos_wide - back_half * sin_wide).reshape(
        row_count, head_count, 2, 1, quarter
    )
    new_back = (front_half * sin_wide + back_half * cos_wide).reshape(
        row_count, head_count, 2, 1, quarter
    )
    return jnp.concatenate([new_front, new_back], axis=3).reshape(row_count, head_count, HEAD_SIZE)


def exchange(block, axis, call_id, gather):
    count = lax.axis_size(axis)
    if count == 1:
        return block[None] if gather else block
    shape = (count,) + block.shape if gather else block.shape

    def kernel(in_ref, out_ref, send_sems, recv_sems, own_sem):
        me = lax.axis_index(axis)
        barrier = pltpu.get_barrier_semaphore()
        for step in range(1, count):
            pl.semaphore_signal(
                barrier,
                inc=1,
                device_id={axis: lax.rem(me + step, count)},
                device_id_type=pl.DeviceIdType.MESH,
            )
        own = pltpu.make_async_copy(in_ref if gather else in_ref.at[me], out_ref.at[me], own_sem)
        own.start()
        pl.semaphore_wait(barrier, count - 1)
        copies = []
        for step in range(1, count):
            peer = lax.rem(me + step, count)
            copy = pltpu.make_async_remote_copy(
                src_ref=in_ref if gather else in_ref.at[peer],
                dst_ref=out_ref.at[me],
                send_sem=send_sems.at[step],
                recv_sem=recv_sems.at[step],
                device_id={axis: peer},
                device_id_type=pl.DeviceIdType.MESH,
            )
            copy.start()
            copies.append(copy)
        own.wait()
        for copy in copies:
            copy.wait()

    return pl.pallas_call(
        kernel,
        out_shape=jax.ShapeDtypeStruct(shape, block.dtype),
        in_specs=[pl.BlockSpec(memory_space=pltpu.VMEM)],
        out_specs=pl.BlockSpec(memory_space=pltpu.VMEM),
        scratch_shapes=[
            pltpu.SemaphoreType.DMA((count,)),
            pltpu.SemaphoreType.DMA((count,)),
            pltpu.SemaphoreType.DMA,
        ],
        compiler_params=pltpu.CompilerParams(collective_id=call_id, has_side_effects=True),
        name="exchange_%d" % call_id,
    )(block)


def key_block_rows(piece_rows):
    return max((width for width in range(1, 2049) if piece_rows % width == 0))


MESH = pl.DeviceIdType.MESH
COLUMNS = 512
FLIPS = ((1, 2), (1, 3), (0, 2), (0, 3), (1, 0), (1, 1), (0, 1))
TP_FLIPS = (2, 3, 1)


def remote(source, target, send_sem, recv_sem, device):
    return pltpu.make_async_remote_copy(
        src_ref=source,
        dst_ref=target,
        send_sem=send_sem,
        recv_sem=recv_sem,
        device_id=device,
        device_id_type=MESH,
    )


def whole_layer(
    queries_t,
    own_kv,
    own_table,
    gain,
    ffn_gain,
    residual,
    weights,
    tokens,
    capacity,
    topk,
    width,
    tp_count,
    call_id,
):
    count = lax.axis_size("sp")
    planes = count // width
    group = width * tp_count
    span = queries_t.shape[1]
    heads = gain.shape[1] // HEAD_SIZE
    features = heads * HEAD_SIZE
    model = residual.shape[1]
    quarter = model // tp_count
    rows_each = tokens // tp_count
    chunk = 256
    lane_groups = -(-tokens // 128)
    lanes = 128 * lane_groups
    table_rows = own_table.shape[0]
    table_step = table_rows // lane_groups
    slots = group * capacity
    out_proj, gate_w, up_w, down_w, shared_gate, shared_up, shared_down = weights
    hidden_units = gate_w.shape[1]
    shared_units = shared_gate.shape[1]
    pair = width * capacity
    half = tokens // 2
    bf16, f32 = jnp.bfloat16, jnp.float32

    def kernel(
        q_ref, own_ref, tab_ref, gain_ref, ffn_ref, resid_ref, wo_hbm, wg_hbm, wu_hbm, wd_hbm,
        sg_hbm, su_hbm, sd_hbm, out_ref,
        kv, tabs, top, norm, acc, tri, ranks, scales, sel, sel_t, rblk, hblk, rpack, hpack,
        xr, xh, hs, ns, ret, rr, passed, arrived, base, fin, hg, own_hid, si, sdq,
        res, wo, wg, wu, wd, sg, su,
        w_sem, k_sem, tb_send, tb_recv, kz_send, kx_send, k_recv,
        rz_send, rz_recv, ri_send, ri_recv, hz_send, hz_recv, hi_send, hi_recv,
        hg_send, hg_recv, sd_send, sd_recv, si_send, si_recv,
        rt_send, rt_recv, zr_send, zr_recv, f_send, f_recv,
    ):
        me, t = lax.axis_index("sp"), lax.axis_index("tp")
        z, x = me // width, me % width
        p = x * tp_count + t
        side = z // 2
        inner = jnp.where((z == 1) | (z == 2), 1, 0)

        def nearest(k):
            near = k + inner * (1 - 2 * k) if k < 2 else k
            return near + side * (planes - 1 - 2 * near)

        def mate(dx, dt):
            x2 = 1 - x if dx else x
            t2 = t
            if dt & 2:
                t2 = t2 + 2 * (1 - 2 * (t // 2))
            if dt & 1:
                t2 = t2 + (1 - 2 * (t % 2))
            return x2, t2

        def at(plane, x2, t2):
            return {"sp": plane * width + x2, "tp": t2}

        arrived[...] = jnp.zeros(arrived.shape, bf16)
        barrier = pltpu.get_barrier_semaphore()
        for dx, dt in FLIPS:
            pl.semaphore_signal(barrier, inc=1, device_id=at(z, *mate(dx, dt)), device_id_type=MESH)
        for step in range(1, planes):
            for x2 in (x, 1 - x):
                pl.semaphore_signal(
                    barrier, inc=1, device_id=at(lax.rem(z + step, planes), x2, t),
                    device_id_type=MESH,
                )

        def columns(index, size):
            return pl.ds(pl.multiple_of(index * size, 128), size)

        locals_ = [
            pltpu.make_async_copy(resid_ref.at[:, columns(t, quarter)], rblk.at[z], k_sem.at[1]),
            pltpu.make_async_copy(own_ref, kv.at[me], k_sem.at[0]),
            pltpu.make_async_copy(tab_ref, tabs.at[me], k_sem.at[2]),
        ]
        for copy in locals_:
            copy.start()
        loads = [
            pltpu.make_async_copy(source, target, w_sem.at[i])
            for i, (source, target) in enumerate(
                [
                    (wo_hbm, wo), (wg_hbm, wg), (wu_hbm, wu), (wd_hbm, wd),
                    (sg_hbm, sg), (su_hbm, su), (resid_ref, res),
                ]
            )
        ]
        before = lax.broadcasted_iota(jnp.int32, (lanes, lanes), 0)
        after = lax.broadcasted_iota(jnp.int32, (lanes, lanes), 1)
        tri[...] = jnp.where(before < after, 1.0, 0.0).astype(bf16)
        for copy in locals_:
            copy.wait()
        pl.semaphore_wait(barrier, len(FLIPS) + 2 * (planes - 1))

        def along(k):
            return remote(
                own_ref, kv.at[me], kz_send.at[k], k_recv.at[me], at(nearest(k), x, t)
            )

        def table_copy(k, far):
            i = 2 * k + far
            return remote(
                tab_ref, tabs.at[me], tb_send.at[i], tb_recv.at[me],
                at(nearest(k), 1 - x if far else x, t),
            )

        def told(slot):
            return remote(tab_ref, tabs.at[slot], tb_send.at[1], tb_recv.at[slot], at(z, 1 - x, t))

        def came(slot):
            return remote(own_ref, kv.at[slot], kz_send.at[0], k_recv.at[slot], at(z, 1 - x, t))

        def across(plane):
            slot = plane * width + x
            return remote(kv.at[slot], kv.at[slot], kx_send.at[plane], k_recv.at[slot], at(z, 1 - x, t))

        def z_hop(blk, b, up, ssem, rsem):
            return remote(
                blk.at[b], blk.at[b], ssem.at[up, b], rsem.at[b],
                at(z + (1 if up else -1), x, t),
            )

        def goes(b, up):
            return (b <= z) & (z < planes - 1) if up else (b >= z) & (z > 0)

        def forward(blk, b, ssem, rsem):
            for up in (1, 0):
                @pl.when(goes(b, up))
                def _():
                    z_hop(blk, b, up, ssem, rsem).start()

        def landed(b, wide, dst, x2, t2):
            return dst.at[b * width + x2, :, columns(t2, wide)]

        def deal_copy(b, pack, dst, wide, ssem, rsem, i):
            x2, t2 = mate(*FLIPS[i])
            rows = pl.ds(pl.multiple_of((x2 * tp_count + t2) * capacity, 16), capacity)
            return remote(
                pack.at[b, rows], landed(b, wide, dst, x, t), ssem.at[b, i], rsem.at[b, i],
                at(z, x2, t2),
            )

        def deal_own(b, pack, dst, wide, rsem):
            rows = pl.ds(pl.multiple_of(p * capacity, 16), capacity)
            return pltpu.make_async_copy(
                pack.at[b, rows], landed(b, wide, dst, x, t), rsem.at[b, len(FLIPS)]
            )

        def deal(b, blk, pack, dst, wide, ssem, rsem):
            for start in range(0, slots, tokens):
                pack[b, start : start + tokens, :] = jnp.dot(
                    sel[b, start : start + tokens, 0:tokens], blk[b], preferred_element_type=f32
                ).astype(bf16)
            for i in range(len(FLIPS)):
                deal_copy(b, pack, dst, wide, ssem, rsem, i).start()
            deal_own(b, pack, dst, wide, rsem).start()

        def dealt(b, pack, dst, wide, ssem, rsem):
            for i in range(len(FLIPS)):
                x2, t2 = mate(*FLIPS[i])
                remote(
                    pack.at[b, 0:capacity], landed(b, wide, dst, x2, t2), ssem.at[b, i],
                    rsem.at[b, i], at(z, x2, t2),
                ).wait_recv()
            deal_own(b, pack, dst, wide, rsem).wait()

        resid_path = (rblk, rpack, xr, quarter, ri_send, ri_recv)
        heads_path = (hblk, hpack, xh, features, hi_send, hi_recv)

        def table(slot):
            return tabs[slot].astype(f32)

        def index(b):
            rows = table(b * width + x)
            named = (lax.broadcasted_iota(jnp.int32, (group, 128), 0) + z * group).astype(f32)
            for j in range(lane_groups):
                hit = jnp.zeros((group, 128), f32)
                for k in range(topk):
                    row = rows[j * table_step + k : j * table_step + k + 1]
                    hit = jnp.where(row == named, 1.0, hit)
                ranks[0:group, 128 * j : 128 * j + 128] = hit
            member = ranks[0:group, :]
            rank = jnp.dot(member.astype(bf16), tri[...], preferred_element_type=f32)
            ranks[0:group, :] = jnp.where(member > 0.5, rank, -1.0)
            wanted = lax.broadcasted_iota(jnp.int32, (capacity, 128), 0).astype(f32)
            for e in range(group):
                for j in range(lane_groups):
                    row = ranks[e : e + 1, 128 * j : 128 * j + 128]
                    sel[b, e * capacity : (e + 1) * capacity, 128 * j : 128 * j + 128] = jnp.where(
                        row == wanted, 1.0, 0.0
                    ).astype(bf16)

        def weigh(slot, carry):
            rows = table(slot)
            mine_is = (z * group + p).astype(f32)
            amounts = []
            for j in range(lane_groups):
                hit = jnp.zeros((1, 128), f32)
                amount = jnp.zeros((1, 128), f32)
                for k in range(topk):
                    at_row = j * table_step + k
                    same = rows[at_row : at_row + 1] == mine_is
                    high = rows[at_row + topk : at_row + topk + 1]
                    low = rows[at_row + 2 * topk : at_row + 2 * topk + 1]
                    hit = jnp.where(same, 1.0, hit)
                    amount = jnp.where(same, high + low, amount)
                ranks[0:8, 128 * j : 128 * j + 128] = jnp.broadcast_to(hit, (8, 128))
                amounts.append(amount)
            member = ranks[0:8, :]
            rank = jnp.dot(member.astype(bf16), tri[...], preferred_element_type=f32)
            ranks[0:8, :] = jnp.where(member > 0.5, rank, -1.0)
            wanted = lax.broadcasted_iota(jnp.int32, (capacity, 128), 0).astype(f32)
            summed = jnp.zeros((capacity, 128), f32)
            for j in range(lane_groups):
                row = ranks[0:1, 128 * j : 128 * j + 128]
                summed = summed + jnp.where(row == wanted, amounts[j], 0.0)
            scales[slot] = jnp.broadcast_to(
                jnp.sum(summed, axis=1, keepdims=True), (capacity, 128)
            )
            return carry

        def absorb(slot):
            keys = kv[slot, 0:tokens, 0:HEAD_SIZE]
            vals_t = kv[slot, 0:tokens, HEAD_SIZE : 2 * HEAD_SIZE].T
            for start in range(0, span, chunk):
                part = pl.ds(start, chunk)
                scores = jnp.dot(keys, q_ref[:, part], preferred_element_type=f32)
                old = top[:, part]
                peak = jnp.maximum(old, jnp.max(scores, axis=0, keepdims=True))
                factor = jnp.exp(old - peak)
                terms = jnp.exp(scores - peak)
                norm[:, part] = norm[:, part] * factor + jnp.sum(terms, axis=0, keepdims=True)
                acc[:, part] = acc[:, part] * factor + jnp.dot(
                    vals_t, terms.astype(bf16), preferred_element_type=f32
                )
                top[:, part] = peak

        def each_side(step, body):
            def side_of(i, carry):
                b = z + (2 * i - 1) * step

                @pl.when((b >= 0) & (b < planes))
                def _():
                    body(b)

                return carry

            lax.fori_loop(0, 2, side_of, 0)

        def pass_resid(step):
            def body(b):
                z_hop(rblk, b, 0, rz_send, rz_recv).wait_recv()
                forward(rblk, b, rz_send, rz_recv)
                told(b * width + x).wait_recv()
                index(b)
                deal(b, *resid_path)

            each_side(step, body)

        def pass_heads(step):
            def body(b):
                z_hop(hblk, b, 0, hz_send, hz_recv).wait_recv()
                forward(hblk, b, hz_send, hz_recv)
                deal(b, *heads_path)

            each_side(step, body)

        for k in range(1, planes):
            table_copy(k, 0).start()
        for k in range(1, planes):
            along(k).start()
        across(z).start()
        forward(rblk, z, rz_send, rz_recv)
        for k in range(planes):
            table_copy(k, 1).start()
        index(z)
        deal(z, *resid_path)
        for load in loads:
            load.start()
        sd_copies = []
        for i, dt in enumerate(TP_FLIPS):
            _, t2 = mate(0, dt)
            copy = remote(
                sd_hbm.at[:, columns(t2, quarter)],
                sdq.at[pl.ds(pl.multiple_of(t * shared_units, 16), shared_units)],
                sd_send.at[i], sd_recv.at[i], at(z, x, t2),
            )
            copy.start()
            sd_copies.append(copy)
        sd_own = pltpu.make_async_copy(
            sd_hbm.at[:, columns(t, quarter)],
            sdq.at[pl.ds(pl.multiple_of(t * shared_units, 16), shared_units)],
            sd_recv.at[len(TP_FLIPS)],
        )
        sd_own.start()
        top[...] = jnp.full(top.shape, -1e30, f32)
        norm[...] = jnp.zeros(norm.shape, f32)
        acc[...] = jnp.zeros(acc.shape, f32)
        absorb(me)

        def attend(k, far):
            slot = nearest(k) * width + ((1 - x) if far else x)
            came(slot).wait_recv()
            if not far:
                across(nearest(k)).start()
            absorb(slot)

        for k in range(1, planes):
            attend(k, False)
        attend(0, True)
        attend(1, True)
        pass_resid(1)
        attend(2, True)
        attend(3, True)

        attended = acc[...] / norm[...]
        mean_sq = jnp.mean(attended * attended, axis=0, keepdims=True)
        rows = (attended * lax.rsqrt(mean_sq + EPS)).T
        for h in range(heads):
            hblk[z, :, h * HEAD_SIZE : (h + 1) * HEAD_SIZE] = (
                rows[h * tokens : (h + 1) * tokens]
                * gain_ref[:, h * HEAD_SIZE : (h + 1) * HEAD_SIZE]
            ).astype(bf16)

        forward(hblk, z, hz_send, hz_recv)
        deal(z, *heads_path)

        def gather(i):
            _, t2 = mate(0, TP_FLIPS[i])
            if i == 1:
                _, t3 = mate(0, 2)
                _, t2 = mate(0, 1)
                rows = hg.at[:, columns(t3, features)]
                return remote(rows, rows, hg_send.at[i], hg_recv.at[i], at(z, x, t2))
            return remote(
                hblk.at[z], hg.at[:, columns(t, features)], hg_send.at[i], hg_recv.at[i],
                at(z, x, t2),
            )

        hg_own = pltpu.make_async_copy(
            hblk.at[z], hg.at[:, columns(t, features)], hg_recv.at[len(TP_FLIPS)]
        )
        hg_own.start()

        def normalize(head_rows, resid_at):
            count_rows = head_rows.shape[0]
            squares = jnp.zeros((count_rows, 1), f32)
            for start in range(0, model, COLUMNS):
                part = slice(start, start + COLUMNS)
                field = jnp.dot(head_rows, wo[:, part], preferred_element_type=f32)
                field = (resid_at(part).astype(f32) + field).astype(bf16)
                hs[:, part] = field
                field = field.astype(f32)
                squares = squares + jnp.sum(field * field, axis=1, keepdims=True)
            inverse = lax.rsqrt(squares / model + EPS)
            for start in range(0, model, COLUMNS):
                part = slice(start, start + COLUMNS)
                ns[:, part] = (hs[:, part].astype(f32) * inverse * ffn_ref[:, part]).astype(bf16)

        def glu(gate_ref, up_ref):
            gate = jnp.dot(ns[...], gate_ref[...], preferred_element_type=f32)
            up = jnp.dot(ns[...], up_ref[...], preferred_element_type=f32)
            return (gate / (1.0 + jnp.exp(-gate)) * up).astype(bf16)

        def back_copy(b, j, i):
            x2, t2 = mate(*FLIPS[i])
            return remote(
                ret.at[b * width + x2, :, columns(t2, quarter)], rr.at[b, p],
                rt_send.at[b, i], rt_recv.at[b, i], at(z, x2, t2),
            )

        def back_own(b):
            return pltpu.make_async_copy(
                ret.at[b * width + x, :, columns(t, quarter)], rr.at[b, p],
                rt_recv.at[b, len(FLIPS)],
            )

        def expert(k):
            b = nearest(k)
            dealt(b, *resid_path[1:])
            dealt(b, *heads_path[1:])
            both = pl.ds(b * width, width)

            def resid_at(part):
                return xr[both, :, part].reshape(pair, COLUMNS)

            normalize(xh[both].reshape(pair, tp_count * features), resid_at)
            inner_rows = glu(wg, wu)
            scale = scales[both].reshape(pair, 128)[:, 0:1]
            for start in range(0, model, COLUMNS):
                part = slice(start, start + COLUMNS)
                made = jnp.dot(inner_rows, wd[:, part], preferred_element_type=f32) * scale
                ret[both, :, part] = made.astype(bf16).reshape(width, capacity, COLUMNS)

        def give_back(k):
            b = nearest(k)
            for i in range(len(FLIPS)):
                back_copy(b, 0, i).start()
            back_own(b).start()

        def given(k):
            for i in range(len(FLIPS)):
                back_copy(nearest(k), 0, i).wait_send()

        def inner_copy(i):
            _, t2 = mate(0, TP_FLIPS[i])
            return remote(
                si.at[:, columns(t, shared_units)], si.at[:, columns(t, shared_units)],
                si_send.at[i], si_recv.at[i], at(z, x, t2),
            )

        def shared_inner():
            for i in range(len(TP_FLIPS)):
                _, t2 = mate(0, TP_FLIPS[i])
                remote(
                    hblk.at[z], hg.at[:, columns(t2, features)], hg_send.at[i], hg_recv.at[i],
                    at(z, x, t2),
                ).wait_recv()
                if i == 0:
                    gather(1).start()
            hg_own.wait()
            for start in (0, half):
                span_rows = slice(start, start + half)
                normalize(hg[span_rows, :], lambda part: res[span_rows, part])
                own_hid[span_rows, :] = hs[:, columns(t, quarter)]
                si[span_rows, columns(t, shared_units)] = glu(sg, su)
            for i in range(len(TP_FLIPS)):
                inner_copy(i).start()

        def shared_out():
            for i in range(len(TP_FLIPS)):
                _, t2 = mate(0, TP_FLIPS[i])
                remote(
                    si.at[:, columns(t, shared_units)], si.at[:, columns(t2, shared_units)],
                    si_send.at[i], si_recv.at[i], at(z, x, t2),
                ).wait_recv()
                remote(
                    sd_hbm.at[:, columns(t2, quarter)],
                    sdq.at[pl.ds(pl.multiple_of(t2 * shared_units, 16), shared_units)],
                    sd_send.at[i], sd_recv.at[i], at(z, x, t2),
                ).wait_recv()
            sd_own.wait()
            base[...] = own_hid[...].astype(f32) + jnp.dot(
                si[...], sdq[...], preferred_element_type=f32
            )

        pass_resid(2)
        pass_heads(1)
        for i in (0, 2):
            gather(i).start()
        pass_resid(3)
        pass_heads(2)
        pass_heads(3)
        for step in range(planes):
            told(step * width + (1 - x)).wait_recv()
        lax.fori_loop(0, count, weigh, 0)
        for load in loads:
            load.wait()
        expert(0)
        expert(1)
        shared_inner()
        expert(3)
        give_back(3)
        expert(2)
        given(3)
        give_back(2)

        cuts = [slice(start, start + 256) for start in range(0, quarter, 256)]

        def down_hop(b, c, down):
            return remote(
                passed.at[b, :, cuts[c]], arrived.at[down, b, :, cuts[c]],
                zr_send.at[b, c], zr_recv.at[down, b, c],
                at(z + (-1 if down else 1), x, t),
            )

        def owner_copy(c, i):
            _, t2 = mate(0, TP_FLIPS[i])
            rows = pl.ds(pl.multiple_of(t2 * rows_each, 16), rows_each)
            return remote(
                fin.at[rows, cuts[c]],
                out_ref.at[:, pl.ds(pl.multiple_of(t * quarter + 256 * c, 128), 256)],
                f_send.at[c, i], f_recv.at[c, i], at(z, x, t2),
            )

        def owner_own(c):
            rows = pl.ds(pl.multiple_of(t * rows_each, 16), rows_each)
            return pltpu.make_async_copy(
                fin.at[rows, cuts[c]],
                out_ref.at[:, pl.ds(pl.multiple_of(t * quarter + 256 * c, 128), 256)],
                f_recv.at[c, len(TP_FLIPS)],
            )

        def combine(k):
            b = nearest(k)
            for i in range(len(FLIPS)):
                x2, t2 = mate(*FLIPS[i])
                remote(
                    ret.at[0, :, columns(t2, quarter)], rr.at[b, x2 * tp_count + t2],
                    rt_send.at[b, i], rt_recv.at[b, i], at(z, x2, t2),
                ).wait_recv()
            back_own(b).wait()
            sel_t[...] = sel[b, :, 0:tokens].T
            for c, cut in enumerate(cuts):
                @pl.when((z >= b) & (z < planes - 1))
                def _():
                    down_hop(b, c, 1).wait_recv()

                @pl.when((z <= b) & (z > 0))
                def _():
                    down_hop(b, c, 0).wait_recv()

                total = jnp.dot(
                    sel_t[...], rr[b, :, :, cut].reshape(slots, 256), preferred_element_type=f32
                )
                total = total + arrived[1, b, :, cut].astype(f32)
                total = total + arrived[0, b, :, cut].astype(f32)
                if k:
                    passed[b, :, cut] = total.astype(bf16)

                    @pl.when(z > b)
                    def _():
                        down_hop(b, c, 1).start()

                    @pl.when(z < b)
                    def _():
                        down_hop(b, c, 0).start()
                else:
                    fin[:, cut] = (total + base[:, cut]).astype(bf16)
                    for i in range(len(TP_FLIPS)):
                        owner_copy(c, i).start()
                    owner_own(c).start()

        combine(3)
        given(2)
        give_back(1)
        combine(2)
        given(1)
        give_back(0)
        combine(1)
        shared_out()
        combine(0)

        for c in range(len(cuts)):
            for i in range(len(TP_FLIPS)):
                _, t2 = mate(0, TP_FLIPS[i])
                remote(
                    fin.at[0:rows_each, cuts[c]],
                    out_ref.at[:, pl.ds(pl.multiple_of(t2 * quarter + 256 * c, 128), 256)],
                    f_send.at[c, i], f_recv.at[c, i], at(z, x, t2),
                ).wait_recv()
            owner_own(c).wait()

        for step in range(1, planes):
            along(step).wait_send()
            table_copy(step, 0).wait_send()
        for k in range(planes):
            b = nearest(k)
            across(b).wait_send()
            table_copy(k, 1).wait_send()
            for up in (1, 0):
                @pl.when(goes(b, up))
                def _():
                    z_hop(rblk, b, up, rz_send, rz_recv).wait_send()
                    z_hop(hblk, b, up, hz_send, hz_recv).wait_send()
            for i in range(len(FLIPS)):
                deal_copy(b, *resid_path[1:], i).wait_send()
                deal_copy(b, *heads_path[1:], i).wait_send()
                if k == 0:
                    back_copy(b, 0, i).wait_send()
            if k:
                for c in range(len(cuts)):
                    down_hop(b, c, 0).wait_send()
        for i in range(len(TP_FLIPS)):
            sd_copies[i].wait_send()
            gather(i).wait_send()
            inner_copy(i).wait_send()
            for c in range(len(cuts)):
                owner_copy(c, i).wait_send()

    vmem = pl.BlockSpec(memory_space=pltpu.VMEM)
    anywhere = pl.BlockSpec(memory_space=pl.ANY)
    dma = pltpu.SemaphoreType.DMA
    flips, tps = len(FLIPS), len(TP_FLIPS)
    cut_count = quarter // 256
    return pl.pallas_call(
        kernel,
        out_shape=jax.ShapeDtypeStruct((rows_each, model), bf16),
        in_specs=[vmem] * 5 + [anywhere] * 8,
        out_specs=vmem,
        scratch_shapes=[
            pltpu.VMEM((count,) + own_kv.shape, bf16),
            pltpu.VMEM((count,) + own_table.shape, bf16),
            pltpu.VMEM((1, span), f32),
            pltpu.VMEM((1, span), f32),
            pltpu.VMEM((HEAD_SIZE, span), f32),
            pltpu.VMEM((lanes, lanes), bf16),
            pltpu.VMEM((group, lanes), f32),
            pltpu.VMEM((count, capacity, 128), f32),
            pltpu.VMEM((planes, slots, lanes), bf16),
            pltpu.VMEM((tokens, slots), bf16),
            pltpu.VMEM((planes, tokens, quarter), bf16),
            pltpu.VMEM((planes, tokens, features), bf16),
            pltpu.VMEM((planes, slots, quarter), bf16),
            pltpu.VMEM((planes, slots, features), bf16),
            pltpu.VMEM((count, capacity, model), bf16),
            pltpu.VMEM((count, capacity, tp_count * features), bf16),
            pltpu.VMEM((pair, model), bf16),
            pltpu.VMEM((pair, model), bf16),
            pltpu.VMEM((count, capacity, model), bf16),
            pltpu.VMEM((planes, group, capacity, quarter), bf16),
            pltpu.VMEM((planes, tokens, quarter), bf16),
            pltpu.VMEM((2, planes, tokens, quarter), bf16),
            pltpu.VMEM((tokens, quarter), f32),
            pltpu.VMEM((tokens, quarter), bf16),
            pltpu.VMEM((tokens, tp_count * features), bf16),
            pltpu.VMEM((tokens, quarter), bf16),
            pltpu.VMEM((tokens, tp_count * shared_units), bf16),
            pltpu.VMEM((tp_count * shared_units, quarter), bf16),
            pltpu.VMEM(residual.shape, bf16),
            pltpu.VMEM(out_proj.shape, bf16),
            pltpu.VMEM(gate_w.shape, bf16),
            pltpu.VMEM(up_w.shape, bf16),
            pltpu.VMEM(down_w.shape, bf16),
            pltpu.VMEM(shared_gate.shape, bf16),
            pltpu.VMEM(shared_up.shape, bf16),
            dma((7,)),
            dma((3,)),
            dma((2 * planes,)),
            dma((count,)),
            dma((planes,)),
            dma((planes,)),
            dma((count,)),
            dma((2, planes)),
            dma((planes,)),
            dma((planes, flips)),
            dma((planes, flips + 1)),
            dma((2, planes)),
            dma((planes,)),
            dma((planes, flips)),
            dma((planes, flips + 1)),
            dma((tps,)),
            dma((tps + 1,)),
            dma((tps,)),
            dma((tps + 1,)),
            dma((tps,)),
            dma((tps,)),
            dma((planes, flips)),
            dma((planes, flips + 1)),
            dma((planes, cut_count)),
            dma((2, planes, cut_count)),
            dma((cut_count, tps)),
            dma((cut_count, tps + 1)),
        ],
        compiler_params=pltpu.CompilerParams(
            collective_id=call_id, has_side_effects=True, vmem_limit_bytes=63 * 1024 * 1024
        ),
        name="whole_layer",
    )(queries_t, own_kv, own_table, gain, ffn_gain, residual, *weights)


def scan_attention(query_rows, key_blocks, score_scale):
    start_state = (
        jnp.full((query_rows.shape[0],), -1e30, jnp.float32),
        jnp.zeros((query_rows.shape[0],), jnp.float32),
        jnp.zeros(query_rows.shape, jnp.float32),
    )

    def step(carry, key_slab):
        run_max, run_total, run_acc = carry
        scores = (
            lax.dot_general(
                query_rows,
                key_slab[:, :HEAD_SIZE],
                (((1,), (1,)), ((), ())),
                preferred_element_type=jnp.float32,
            )
            * score_scale
        )
        new_max = jnp.maximum(run_max, jnp.max(scores, axis=1))
        factor = jnp.exp(run_max - new_max)
        expo_terms = jnp.exp(scores - new_max[:, None])
        new_total = run_total * factor + jnp.sum(expo_terms, axis=1)
        new_acc = run_acc * factor[:, None] + jnp.dot(
            expo_terms.astype(jnp.bfloat16),
            key_slab[:, HEAD_SIZE:],
            preferred_element_type=jnp.float32,
        )
        return ((new_max, new_total, new_acc), None)

    (_, run_total, run_acc), _ = lax.scan(step, start_state, key_blocks)
    return run_acc / run_total[:, None]


def slot_ranks(member):
    order = jnp.arange(member.shape[0], dtype=jnp.int32)
    before = (order[:, None] > order[None, :]).astype(jnp.bfloat16)
    rank = jnp.dot(before, member.astype(jnp.bfloat16), preferred_element_type=jnp.float32)
    return jnp.where(member, rank.astype(jnp.int32), -1)


def expert_block(flat_rows, gate_local, up_local, down_local):
    gate_out = jnp.dot(flat_rows, gate_local, preferred_element_type=jnp.float32)
    up_out = jnp.dot(flat_rows, up_local, preferred_element_type=jnp.float32)
    expert_inner = (jax.nn.silu(gate_out) * up_out).astype(jnp.bfloat16)
    return jnp.dot(expert_inner, down_local, preferred_element_type=jnp.float32).astype(
        jnp.bfloat16
    )


def local(
    queries,
    key_matrix,
    values,
    query_gain,
    key_norm_gain,
    head_gain,
    out_proj,
    residual,
    ffn_gain,
    routes,
    route_weights,
    expert_gate,
    expert_up,
    expert_down,
    shared_gate,
    shared_up,
    shared_down,
):
    tok_count = queries.shape[0]
    head_count = queries.shape[1] // HEAD_SIZE
    sp_count = lax.axis_size("sp")
    tp_count = lax.axis_size("tp")
    tp_index = lax.axis_index("tp")
    sequence_total = tok_count * sp_count
    positions = lax.axis_index("sp") * tok_count + jnp.arange(tok_count, dtype=jnp.int32)
    cosine_table, sine_table = grid_tables(positions, sequence_total)
    rotated_query = apply_rotary(
        final_norm(
            queries.astype(jnp.float32).reshape(tok_count, head_count, HEAD_SIZE), query_gain
        ),
        cosine_table,
        sine_table,
    ).astype(jnp.bfloat16)
    rotated_key = (
        apply_rotary(
            final_norm(
                key_matrix.astype(jnp.float32).reshape(tok_count, 1, HEAD_SIZE), key_norm_gain
            ),
            cosine_table,
            sine_table,
        )
        .reshape(tok_count, HEAD_SIZE)
        .astype(jnp.bfloat16)
    )
    packed = jnp.concatenate([rotated_key, values], axis=1)
    score_scale = HEAD_SIZE ** (-0.5)
    topk_count = routes.shape[1]
    capacity = max(2, 2 * tok_count * topk_count // (sp_count * tp_count))
    lanes = 2 * HEAD_SIZE
    entries = tok_count * topk_count
    relayed = (
        tp_count == 4
        and sp_count == 2 * tp_count
        and capacity % 16 == 0
        and tok_count % (16 * tp_count) == 0
        and entries % lanes == 0
        and head_count * tok_count % 256 == 0
        and head_count % 2 == 0
    )
    if relayed:
        lane_total = -(-tok_count // 128) * 128
        scale_hi = lax.reduce_precision(route_weights, 8, 7)
        tables = jnp.concatenate(
            [routes.astype(jnp.float32), scale_hi, route_weights - scale_hi], axis=1
        ).T
        tables = jnp.pad(
            tables, ((0, -3 * topk_count % 16), (0, lane_total - tok_count)), constant_values=-1.0
        ).astype(jnp.bfloat16)
        tables = tables.reshape(tables.shape[0], -1, 128).transpose(1, 0, 2).reshape(-1, 128)
        scaled = rotated_query * jnp.asarray(score_scale, jnp.bfloat16)
        return whole_layer(
            scaled.transpose(2, 1, 0).reshape(HEAD_SIZE, head_count * tok_count),
            packed,
            tables,
            head_gain.reshape(1, -1),
            ffn_gain.reshape(1, -1),
            residual,
            (out_proj, expert_gate[0], expert_up[0], expert_down[0], shared_gate, shared_up, shared_down),
            tok_count,
            capacity,
            topk_count,
            sp_count // tp_count,
            tp_count,
            0,
        )
    piece = exchange(packed, "sp", 0, True).reshape(sequence_total, lanes)
    query_rows = rotated_query.transpose(1, 0, 2).reshape(head_count * tok_count, HEAD_SIZE)
    block_length = key_block_rows(sequence_total)
    key_blocks = piece.reshape(sequence_total // block_length, block_length, lanes)
    attended = scan_attention(query_rows, key_blocks, score_scale)
    attended = attended.reshape(head_count, tok_count, HEAD_SIZE).transpose(1, 0, 2)
    head_out = final_norm(attended, head_gain.reshape(head_count, HEAD_SIZE))
    head_out = head_out.astype(jnp.bfloat16).reshape(tok_count, head_count * HEAD_SIZE)
    part_rows = tok_count // tp_count
    token_heads = exchange(
        head_out.reshape(tp_count, part_rows, head_count * HEAD_SIZE), "tp", 1, False
    )
    token_heads = token_heads.transpose(1, 0, 2).reshape(part_rows, -1)
    own_resid = lax.dynamic_slice_in_dim(residual, tp_index * part_rows, part_rows, 0)
    hidden_own = (
        own_resid.astype(jnp.float32)
        + jnp.dot(token_heads, out_proj, preferred_element_type=jnp.float32)
    ).astype(jnp.bfloat16)
    normed_own = final_norm(hidden_own.astype(jnp.float32), ffn_gain).astype(jnp.bfloat16)
    model_width = normed_own.shape[1]
    gate_local = expert_gate[0]
    up_local = expert_up[0]
    down_local = expert_down[0]
    normed = exchange(normed_own, "tp", 2, True).reshape(tok_count, model_width)
    slot_total = sp_count * capacity
    experts_here = jnp.arange(sp_count, dtype=jnp.int32) * tp_count + tp_index
    named = routes[:, :, None] == experts_here[None, None, :]
    member = jnp.any(named, axis=1)
    scale = jnp.sum(jnp.where(named, route_weights[:, :, None], 0.0), axis=1)
    rank = slot_ranks(member)
    slots = jnp.arange(capacity, dtype=jnp.int32)
    chosen = rank.T[:, None, :] == slots[None, :, None]
    select = chosen.astype(jnp.bfloat16).reshape(slot_total, tok_count)
    outgoing = jnp.dot(select, normed, preferred_element_type=jnp.float32).astype(jnp.bfloat16)
    arrived = exchange(outgoing.reshape(sp_count, capacity, model_width), "sp", 3, False)
    produced = expert_block(
        arrived.reshape(slot_total, model_width), gate_local, up_local, down_local
    )
    returned = exchange(produced.reshape(sp_count, capacity, model_width), "sp", 4, False).reshape(
        slot_total, model_width
    )
    combine = jnp.where(chosen, scale.T[:, None, :], 0.0).reshape(slot_total, tok_count)
    combine_hi = lax.reduce_precision(combine, 8, 7)
    combine_lo = (combine - combine_hi).astype(jnp.bfloat16)
    combine_hi = combine_hi.astype(jnp.bfloat16)

    def mix(weights):
        return lax.dot_general(
            weights, returned, (((0,), (0,)), ((), ())), preferred_element_type=jnp.float32
        )

    gate_part = jnp.dot(normed, shared_gate, preferred_element_type=jnp.float32)
    up_part = jnp.dot(normed, shared_up, preferred_element_type=jnp.float32)
    shared_inner = (jax.nn.silu(gate_part) * up_part).astype(jnp.bfloat16)
    shares = (
        jnp.dot(shared_inner, shared_down, preferred_element_type=jnp.float32)
        + mix(combine_hi)
        + mix(combine_lo)
    ).astype(jnp.bfloat16)
    shares = exchange(shares.reshape(tp_count, part_rows, model_width), "tp", 5, False)
    mixed_rows = jnp.sum(shares.astype(jnp.float32), axis=0)
    return (hidden_own.astype(jnp.float32) + mixed_rows).astype(jnp.bfloat16)


def solution(mesh):
    placed = (
        P("sp", "tp"),
        P("sp", "tp"),
        P("sp", "tp"),
        P(),
        P(),
        P("tp"),
        P(),
        P("sp", None),
        P(),
        P("sp", None),
        P("sp", None),
        P(("sp", "tp"), None, None),
        P(("sp", "tp"), None, None),
        P(("sp", "tp"), None, None),
        P(None, "tp"),
        P(None, "tp"),
        P("tp", None),
    )
    return jax.shard_map(
        local, mesh=mesh, in_specs=placed, out_specs=P(("sp", "tp"), None), check_vma=False
    )
```

```python
import jax
import jax.numpy as jnp
from jax import lax
from jax.experimental import pallas as pl
from jax.experimental.pallas import tpu as pltpu
from jax.sharding import PartitionSpec as P

HEAD_SIZE = 64
GRID_W = 64


EPS = 1e-06
THETA = 10000.0


def final_norm(field, gain):
    mean_sq = jnp.mean(field * field, axis=-1, keepdims=True)
    return field * lax.rsqrt(mean_sq + EPS) * gain


def grid_tables(positions, sequence_total):
    grid_rows = sequence_total // GRID_W
    row_pos = (positions // GRID_W - grid_rows // 2).astype(jnp.float32)
    col_pos = (positions % GRID_W - GRID_W // 2).astype(jnp.float32)
    quarter = HEAD_SIZE // 4
    inverse = THETA ** (-jnp.arange(quarter, dtype=jnp.float32) / quarter)
    angles = jnp.concatenate([row_pos[:, None] * inverse, col_pos[:, None] * inverse], axis=1)
    return (jnp.cos(angles), jnp.sin(angles))


def apply_rotary(field, cosine_table, sine_table):
    row_count, head_count = (field.shape[0], field.shape[1])
    quarter = HEAD_SIZE // 4
    pieces = field.reshape(row_count, head_count, 2, 2, quarter)
    front_half = pieces[:, :, :, 0, :].reshape(row_count, head_count, 2 * quarter)
    back_half = pieces[:, :, :, 1, :].reshape(row_count, head_count, 2 * quarter)
    cos_wide = cosine_table[:, None, :]
    sin_wide = sine_table[:, None, :]
    new_front = (front_half * cos_wide - back_half * sin_wide).reshape(
        row_count, head_count, 2, 1, quarter
    )
    new_back = (front_half * sin_wide + back_half * cos_wide).reshape(
        row_count, head_count, 2, 1, quarter
    )
    return jnp.concatenate([new_front, new_back], axis=3).reshape(row_count, head_count, HEAD_SIZE)


def exchange(block, axis, call_id, gather):
    count = lax.axis_size(axis)
    if count == 1:
        return block[None] if gather else block
    shape = (count,) + block.shape if gather else block.shape

    def kernel(in_ref, out_ref, send_sems, recv_sems, own_sem):
        me = lax.axis_index(axis)
        barrier = pltpu.get_barrier_semaphore()
        for step in range(1, count):
            pl.semaphore_signal(
                barrier,
                inc=1,
                device_id={axis: lax.rem(me + step, count)},
                device_id_type=pl.DeviceIdType.MESH,
            )
        own = pltpu.make_async_copy(in_ref if gather else in_ref.at[me], out_ref.at[me], own_sem)
        own.start()
        pl.semaphore_wait(barrier, count - 1)
        copies = []
        for step in range(1, count):
            peer = lax.rem(me + step, count)
            copy = pltpu.make_async_remote_copy(
                src_ref=in_ref if gather else in_ref.at[peer],
                dst_ref=out_ref.at[me],
                send_sem=send_sems.at[step],
                recv_sem=recv_sems.at[step],
                device_id={axis: peer},
                device_id_type=pl.DeviceIdType.MESH,
            )
            copy.start()
            copies.append(copy)
        own.wait()
        for copy in copies:
            copy.wait()

    return pl.pallas_call(
        kernel,
        out_shape=jax.ShapeDtypeStruct(shape, block.dtype),
        in_specs=[pl.BlockSpec(memory_space=pltpu.VMEM)],
        out_specs=pl.BlockSpec(memory_space=pltpu.VMEM),
        scratch_shapes=[
            pltpu.SemaphoreType.DMA((count,)),
            pltpu.SemaphoreType.DMA((count,)),
            pltpu.SemaphoreType.DMA,
        ],
        compiler_params=pltpu.CompilerParams(collective_id=call_id, has_side_effects=True),
        name="exchange_%d" % call_id,
    )(block)


def key_block_rows(piece_rows):
    return max((width for width in range(1, 2049) if piece_rows % width == 0))


MESH = pl.DeviceIdType.MESH
COLUMNS = 512
FLIPS = ((1, 2), (1, 3), (0, 2), (0, 3), (1, 0), (1, 1), (0, 1))
TP_FLIPS = (2, 3, 1)


def remote(source, target, send_sem, recv_sem, device):
    return pltpu.make_async_remote_copy(
        src_ref=source,
        dst_ref=target,
        send_sem=send_sem,
        recv_sem=recv_sem,
        device_id=device,
        device_id_type=MESH,
    )


def whole_layer(
    queries_t,
    own_kv,
    own_table,
    gain,
    ffn_gain,
    residual,
    weights,
    tokens,
    capacity,
    topk,
    width,
    tp_count,
    call_id,
):
    count = lax.axis_size("sp")
    planes = count // width
    group = width * tp_count
    span = queries_t.shape[1]
    heads = gain.shape[1] // HEAD_SIZE
    features = heads * HEAD_SIZE
    model = residual.shape[1]
    quarter = model // tp_count
    rows_each = tokens // tp_count
    chunk = 256
    lane_groups = -(-tokens // 128)
    lanes = 128 * lane_groups
    table_rows = own_table.shape[0]
    table_step = table_rows // lane_groups
    slots = group * capacity
    out_proj, gate_w, up_w, down_w, shared_gate, shared_up, shared_down = weights
    hidden_units = gate_w.shape[1]
    shared_units = shared_gate.shape[1]
    pair = width * capacity
    half = tokens // 2
    bf16, f32 = jnp.bfloat16, jnp.float32

    def kernel(
        q_ref, own_ref, tab_ref, gain_ref, ffn_ref, resid_ref, wo_hbm, wg_hbm, wu_hbm, wd_hbm,
        sg_hbm, su_hbm, sd_hbm, out_ref,
        kv, tabs, top, norm, acc, tri, ranks, scales, sel, sel_t, rblk, hblk, rpack, hpack,
        xr, xh, hs, ns, ret, rr, passed, arrived, base, fin, hg, own_hid, si, sdq,
        res, wo, wg, wu, wd, sg, su,
        w_sem, k_sem, tb_send, tb_recv, kz_send, kx_send, k_recv,
        rz_send, rz_recv, ri_send, ri_recv, hz_send, hz_recv, hi_send, hi_recv,
        hg_send, hg_recv, sd_send, sd_recv, si_send, si_recv,
        rt_send, rt_recv, zr_send, zr_recv, f_send, f_recv,
    ):
        me, t = lax.axis_index("sp"), lax.axis_index("tp")
        z, x = me // width, me % width
        p = x * tp_count + t
        side = z // 2
        inner = jnp.where((z == 1) | (z == 2), 1, 0)

        def nearest(k):
            near = k + inner * (1 - 2 * k) if k < 2 else k
            return near + side * (planes - 1 - 2 * near)

        def mate(dx, dt):
            x2 = 1 - x if dx else x
            t2 = t
            if dt & 2:
                t2 = t2 + 2 * (1 - 2 * (t // 2))
            if dt & 1:
                t2 = t2 + (1 - 2 * (t % 2))
            return x2, t2

        def at(plane, x2, t2):
            return {"sp": plane * width + x2, "tp": t2}

        arrived[...] = jnp.zeros(arrived.shape, bf16)
        barrier = pltpu.get_barrier_semaphore()
        for dx, dt in FLIPS:
            pl.semaphore_signal(barrier, inc=1, device_id=at(z, *mate(dx, dt)), device_id_type=MESH)
        for step in range(1, planes):
            for x2 in (x, 1 - x):
                pl.semaphore_signal(
                    barrier, inc=1, device_id=at(lax.rem(z + step, planes), x2, t),
                    device_id_type=MESH,
                )

        def columns(index, size):
            return pl.ds(pl.multiple_of(index * size, 128), size)

        locals_ = [
            pltpu.make_async_copy(resid_ref.at[:, columns(t, quarter)], rblk.at[z], k_sem.at[1]),
            pltpu.make_async_copy(own_ref, kv.at[me], k_sem.at[0]),
            pltpu.make_async_copy(tab_ref, tabs.at[me], k_sem.at[2]),
        ]
        for copy in locals_:
            copy.start()
        loads = [
            pltpu.make_async_copy(source, target, w_sem.at[i])
            for i, (source, target) in enumerate(
                [
                    (wo_hbm, wo), (wg_hbm, wg), (wu_hbm, wu), (wd_hbm, wd),
                    (sg_hbm, sg), (su_hbm, su), (resid_ref, res),
                ]
            )
        ]
        before = lax.broadcasted_iota(jnp.int32, (lanes, lanes), 0)
        after = lax.broadcasted_iota(jnp.int32, (lanes, lanes), 1)
        tri[...] = jnp.where(before < after, 1.0, 0.0).astype(bf16)
        for copy in locals_:
            copy.wait()
        pl.semaphore_wait(barrier, len(FLIPS) + 2 * (planes - 1))

        def along(k):
            return remote(
                own_ref, kv.at[me], kz_send.at[k], k_recv.at[me], at(nearest(k), x, t)
            )

        def table_copy(k, far):
            i = 2 * k + far
            return remote(
                tab_ref, tabs.at[me], tb_send.at[i], tb_recv.at[me],
                at(nearest(k), 1 - x if far else x, t),
            )

        def told(slot):
            return remote(tab_ref, tabs.at[slot], tb_send.at[1], tb_recv.at[slot], at(z, 1 - x, t))

        def came(slot):
            return remote(own_ref, kv.at[slot], kz_send.at[0], k_recv.at[slot], at(z, 1 - x, t))

        def across(plane):
            slot = plane * width + x
            return remote(kv.at[slot], kv.at[slot], kx_send.at[plane], k_recv.at[slot], at(z, 1 - x, t))

        def z_hop(blk, b, up, ssem, rsem):
            return remote(
                blk.at[b], blk.at[b], ssem.at[up, b], rsem.at[b],
                at(z + (1 if up else -1), x, t),
            )

        def goes(b, up):
            return (b <= z) & (z < planes - 1) if up else (b >= z) & (z > 0)

        def forward(blk, b, ssem, rsem):
            for up in (1, 0):
                @pl.when(goes(b, up))
                def _():
                    z_hop(blk, b, up, ssem, rsem).start()

        def landed(b, wide, dst, x2, t2):
            return dst.at[b * width + x2, :, columns(t2, wide)]

        def deal_copy(b, pack, dst, wide, ssem, rsem, i):
            x2, t2 = mate(*FLIPS[i])
            rows = pl.ds(pl.multiple_of((x2 * tp_count + t2) * capacity, 16), capacity)
            return remote(
                pack.at[b, rows], landed(b, wide, dst, x, t), ssem.at[b, i], rsem.at[b, i],
                at(z, x2, t2),
            )

        def deal_own(b, pack, dst, wide, rsem):
            rows = pl.ds(pl.multiple_of(p * capacity, 16), capacity)
            return pltpu.make_async_copy(
                pack.at[b, rows], landed(b, wide, dst, x, t), rsem.at[b, len(FLIPS)]
            )

        def deal(b, blk, pack, dst, wide, ssem, rsem):
            for start in range(0, slots, tokens):
                pack[b, start : start + tokens, :] = jnp.dot(
                    sel[b, start : start + tokens, 0:tokens], blk[b], preferred_element_type=f32
                ).astype(bf16)
            for i in range(len(FLIPS)):
                deal_copy(b, pack, dst, wide, ssem, rsem, i).start()
            deal_own(b, pack, dst, wide, rsem).start()

        def dealt(b, pack, dst, wide, ssem, rsem):
            for i in range(len(FLIPS)):
                x2, t2 = mate(*FLIPS[i])
                remote(
                    pack.at[b, 0:capacity], landed(b, wide, dst, x2, t2), ssem.at[b, i],
                    rsem.at[b, i], at(z, x2, t2),
                ).wait_recv()
            deal_own(b, pack, dst, wide, rsem).wait()

        resid_path = (rblk, rpack, xr, quarter, ri_send, ri_recv)
        heads_path = (hblk, hpack, xh, features, hi_send, hi_recv)

        def table(slot):
            return tabs[slot].astype(f32)

        def index(b):
            rows = table(b * width + x)
            named = (lax.broadcasted_iota(jnp.int32, (group, 128), 0) + z * group).astype(f32)
            for j in range(lane_groups):
                hit = jnp.zeros((group, 128), f32)
                for k in range(topk):
                    row = rows[j * table_step + k : j * table_step + k + 1]
                    hit = jnp.where(row == named, 1.0, hit)
                ranks[0:group, 128 * j : 128 * j + 128] = hit
            member = ranks[0:group, :]
            rank = jnp.dot(member.astype(bf16), tri[...], preferred_element_type=f32)
            ranks[0:group, :] = jnp.where(member > 0.5, rank, -1.0)
            wanted = lax.broadcasted_iota(jnp.int32, (capacity, 128), 0).astype(f32)
            for e in range(group):
                for j in range(lane_groups):
                    row = ranks[e : e + 1, 128 * j : 128 * j + 128]
                    sel[b, e * capacity : (e + 1) * capacity, 128 * j : 128 * j + 128] = jnp.where(
                        row == wanted, 1.0, 0.0
                    ).astype(bf16)

        def weigh(slot, carry):
            rows = table(slot)
            mine_is = (z * group + p).astype(f32)
            amounts = []
            for j in range(lane_groups):
                hit = jnp.zeros((1, 128), f32)
                amount = jnp.zeros((1, 128), f32)
                for k in range(topk):
                    at_row = j * table_step + k
                    same = rows[at_row : at_row + 1] == mine_is
                    high = rows[at_row + topk : at_row + topk + 1]
                    low = rows[at_row + 2 * topk : at_row + 2 * topk + 1]
                    hit = jnp.where(same, 1.0, hit)
                    amount = jnp.where(same, high + low, amount)
                ranks[0:8, 128 * j : 128 * j + 128] = jnp.broadcast_to(hit, (8, 128))
                amounts.append(amount)
            member = ranks[0:8, :]
            rank = jnp.dot(member.astype(bf16), tri[...], preferred_element_type=f32)
            ranks[0:8, :] = jnp.where(member > 0.5, rank, -1.0)
            wanted = lax.broadcasted_iota(jnp.int32, (capacity, 128), 0).astype(f32)
            summed = jnp.zeros((capacity, 128), f32)
            for j in range(lane_groups):
                row = ranks[0:1, 128 * j : 128 * j + 128]
                summed = summed + jnp.where(row == wanted, amounts[j], 0.0)
            scales[slot] = jnp.broadcast_to(
                jnp.sum(summed, axis=1, keepdims=True), (capacity, 128)
            )
            return carry

        def absorb(slot):
            keys = kv[slot, 0:tokens, 0:HEAD_SIZE]
            vals_t = kv[slot, 0:tokens, HEAD_SIZE : 2 * HEAD_SIZE].T
            for start in range(0, span, chunk):
                part = pl.ds(start, chunk)
                scores = jnp.dot(keys, q_ref[:, part], preferred_element_type=f32)
                old = top[:, part]
                peak = jnp.maximum(old, jnp.max(scores, axis=0, keepdims=True))
                factor = jnp.exp(old - peak)
                terms = jnp.exp(scores - peak)
                norm[:, part] = norm[:, part] * factor + jnp.sum(terms, axis=0, keepdims=True)
                acc[:, part] = acc[:, part] * factor + jnp.dot(
                    vals_t, terms.astype(bf16), preferred_element_type=f32
                )
                top[:, part] = peak

        def each_side(step, body):
            def side_of(i, carry):
                b = z + (2 * i - 1) * step

                @pl.when((b >= 0) & (b < planes))
                def _():
                    body(b)

                return carry

            lax.fori_loop(0, 2, side_of, 0)

        def pass_resid(step):
            def body(b):
                z_hop(rblk, b, 0, rz_send, rz_recv).wait_recv()
                forward(rblk, b, rz_send, rz_recv)
                told(b * width + x).wait_recv()
                index(b)
                deal(b, *resid_path)

            each_side(step, body)

        def pass_heads(step):
            def body(b):
                z_hop(hblk, b, 0, hz_send, hz_recv).wait_recv()
                forward(hblk, b, hz_send, hz_recv)
                deal(b, *heads_path)

            each_side(step, body)

        for k in range(1, planes):
            table_copy(k, 0).start()
        for k in range(1, planes):
            along(k).start()
        across(z).start()
        forward(rblk, z, rz_send, rz_recv)
        for k in range(planes):
            table_copy(k, 1).start()
        index(z)
        deal(z, *resid_path)
        for load in loads:
            load.start()
        sd_copies = []
        for i, dt in enumerate(TP_FLIPS):
            _, t2 = mate(0, dt)
            copy = remote(
                sd_hbm.at[:, columns(t2, quarter)],
                sdq.at[pl.ds(pl.multiple_of(t * shared_units, 16), shared_units)],
                sd_send.at[i], sd_recv.at[i], at(z, x, t2),
            )
            copy.start()
            sd_copies.append(copy)
        sd_own = pltpu.make_async_copy(
            sd_hbm.at[:, columns(t, quarter)],
            sdq.at[pl.ds(pl.multiple_of(t * shared_units, 16), shared_units)],
            sd_recv.at[len(TP_FLIPS)],
        )
        sd_own.start()
        top[...] = jnp.full(top.shape, -1e30, f32)
        norm[...] = jnp.zeros(norm.shape, f32)
        acc[...] = jnp.zeros(acc.shape, f32)
        absorb(me)

        def attend(k, far):
            slot = nearest(k) * width + ((1 - x) if far else x)
            came(slot).wait_recv()
            if not far:
                across(nearest(k)).start()
            absorb(slot)

        for k in range(1, planes):
            attend(k, False)
        attend(0, True)
        attend(1, True)
        pass_resid(1)
        attend(2, True)
        attend(3, True)

        attended = acc[...] / norm[...]
        mean_sq = jnp.mean(attended * attended, axis=0, keepdims=True)
        rows = (attended * lax.rsqrt(mean_sq + EPS)).T
        for h in range(heads):
            hblk[z, :, h * HEAD_SIZE : (h + 1) * HEAD_SIZE] = (
                rows[h * tokens : (h + 1) * tokens]
                * gain_ref[:, h * HEAD_SIZE : (h + 1) * HEAD_SIZE]
            ).astype(bf16)

        forward(hblk, z, hz_send, hz_recv)
        deal(z, *heads_path)

        def gather(i):
            _, t2 = mate(0, TP_FLIPS[i])
            if i == 1:
                _, t3 = mate(0, 2)
                _, t2 = mate(0, 1)
                rows = hg.at[:, columns(t3, features)]
                return remote(rows, rows, hg_send.at[i], hg_recv.at[i], at(z, x, t2))
            return remote(
                hblk.at[z], hg.at[:, columns(t, features)], hg_send.at[i], hg_recv.at[i],
                at(z, x, t2),
            )

        hg_own = pltpu.make_async_copy(
            hblk.at[z], hg.at[:, columns(t, features)], hg_recv.at[len(TP_FLIPS)]
        )
        hg_own.start()

        def normalize(head_rows, resid_at):
            count_rows = head_rows.shape[0]
            squares = jnp.zeros((count_rows, 1), f32)
            for start in range(0, model, COLUMNS):
                part = slice(start, start + COLUMNS)
                field = jnp.dot(head_rows, wo[:, part], preferred_element_type=f32)
                field = (resid_at(part).astype(f32) + field).astype(bf16)
                hs[:, part] = field
                field = field.astype(f32)
                squares = squares + jnp.sum(field * field, axis=1, keepdims=True)
            inverse = lax.rsqrt(squares / model + EPS)
            for start in range(0, model, COLUMNS):
                part = slice(start, start + COLUMNS)
                ns[:, part] = (hs[:, part].astype(f32) * inverse * ffn_ref[:, part]).astype(bf16)

        def glu(gate_ref, up_ref):
            gate = jnp.dot(ns[...], gate_ref[...], preferred_element_type=f32)
            up = jnp.dot(ns[...], up_ref[...], preferred_element_type=f32)
            return (gate / (1.0 + jnp.exp(-gate)) * up).astype(bf16)

        def back_copy(b, j, i):
            x2, t2 = mate(*FLIPS[i])
            return remote(
                ret.at[b * width + x2, :, columns(t2, quarter)], rr.at[b, p],
                rt_send.at[b, i], rt_recv.at[b, i], at(z, x2, t2),
            )

        def back_own(b):
            return pltpu.make_async_copy(
                ret.at[b * width + x, :, columns(t, quarter)], rr.at[b, p],
                rt_recv.at[b, len(FLIPS)],
            )

        def expert(k):
            b = nearest(k)
            dealt(b, *resid_path[1:])
            dealt(b, *heads_path[1:])
            both = pl.ds(b * width, width)

            def resid_at(part):
                return xr[both, :, part].reshape(pair, COLUMNS)

            normalize(xh[both].reshape(pair, tp_count * features), resid_at)
            inner_rows = glu(wg, wu)
            scale = scales[both].reshape(pair, 128)[:, 0:1]
            for start in range(0, model, COLUMNS):
                part = slice(start, start + COLUMNS)
                made = jnp.dot(inner_rows, wd[:, part], preferred_element_type=f32) * scale
                ret[both, :, part] = made.astype(bf16).reshape(width, capacity, COLUMNS)

        def give_back(k):
            b = nearest(k)
            for i in range(len(FLIPS)):
                back_copy(b, 0, i).start()
            back_own(b).start()

        def given(k):
            for i in range(len(FLIPS)):
                back_copy(nearest(k), 0, i).wait_send()

        def inner_copy(i):
            _, t2 = mate(0, TP_FLIPS[i])
            return remote(
                si.at[:, columns(t, shared_units)], si.at[:, columns(t, shared_units)],
                si_send.at[i], si_recv.at[i], at(z, x, t2),
            )

        def shared_inner():
            for i in range(len(TP_FLIPS)):
                _, t2 = mate(0, TP_FLIPS[i])
                remote(
                    hblk.at[z], hg.at[:, columns(t2, features)], hg_send.at[i], hg_recv.at[i],
                    at(z, x, t2),
                ).wait_recv()
                if i == 0:
                    gather(1).start()
            hg_own.wait()
            for start in (0, half):
                span_rows = slice(start, start + half)
                normalize(hg[span_rows, :], lambda part: res[span_rows, part])
                own_hid[span_rows, :] = hs[:, columns(t, quarter)]
                si[span_rows, columns(t, shared_units)] = glu(sg, su)
            for i in range(len(TP_FLIPS)):
                inner_copy(i).start()

        def shared_out():
            for i in range(len(TP_FLIPS)):
                _, t2 = mate(0, TP_FLIPS[i])
                remote(
                    si.at[:, columns(t, shared_units)], si.at[:, columns(t2, shared_units)],
                    si_send.at[i], si_recv.at[i], at(z, x, t2),
                ).wait_recv()
                remote(
                    sd_hbm.at[:, columns(t2, quarter)],
                    sdq.at[pl.ds(pl.multiple_of(t2 * shared_units, 16), shared_units)],
                    sd_send.at[i], sd_recv.at[i], at(z, x, t2),
                ).wait_recv()
            sd_own.wait()
            base[...] = own_hid[...].astype(f32) + jnp.dot(
                si[...], sdq[...], preferred_element_type=f32
            )

        pass_resid(2)
        pass_heads(1)
        for i in (0, 2):
            gather(i).start()
        pass_resid(3)
        pass_heads(2)
        pass_heads(3)
        for step in range(planes):
            told(step * width + (1 - x)).wait_recv()
        lax.fori_loop(0, count, weigh, 0)
        for load in loads:
            load.wait()
        expert(0)
        expert(1)
        shared_inner()
        expert(3)
        give_back(3)
        expert(2)
        given(3)
        give_back(2)

        cuts = [slice(start, start + 128) for start in range(0, quarter, 128)]

        def down_hop(b, c, down):
            return remote(
                passed.at[b, :, cuts[c]], arrived.at[down, b, :, cuts[c]],
                zr_send.at[b, c], zr_recv.at[down, b, c],
                at(z + (-1 if down else 1), x, t),
            )

        def owner_copy(c, i):
            _, t2 = mate(0, TP_FLIPS[i])
            rows = pl.ds(pl.multiple_of(t2 * rows_each, 16), rows_each)
            return remote(
                fin.at[rows, cuts[c]],
                out_ref.at[:, pl.ds(pl.multiple_of(t * quarter + 128 * c, 128), 128)],
                f_send.at[c, i], f_recv.at[c, i], at(z, x, t2),
            )

        def owner_own(c):
            rows = pl.ds(pl.multiple_of(t * rows_each, 16), rows_each)
            return pltpu.make_async_copy(
                fin.at[rows, cuts[c]],
                out_ref.at[:, pl.ds(pl.multiple_of(t * quarter + 128 * c, 128), 128)],
                f_recv.at[c, len(TP_FLIPS)],
            )

        def combine(k):
            b = nearest(k)
            for i in range(len(FLIPS)):
                x2, t2 = mate(*FLIPS[i])
                remote(
                    ret.at[0, :, columns(t2, quarter)], rr.at[b, x2 * tp_count + t2],
                    rt_send.at[b, i], rt_recv.at[b, i], at(z, x2, t2),
                ).wait_recv()
            back_own(b).wait()
            sel_t[...] = sel[b, :, 0:tokens].T
            for c, cut in enumerate(cuts):
                @pl.when((z >= b) & (z < planes - 1))
                def _():
                    down_hop(b, c, 1).wait_recv()

                @pl.when((z <= b) & (z > 0))
                def _():
                    down_hop(b, c, 0).wait_recv()

                total = jnp.dot(
                    sel_t[...], rr[b, :, :, cut].reshape(slots, 128), preferred_element_type=f32
                )
                total = total + arrived[1, b, :, cut].astype(f32)
                total = total + arrived[0, b, :, cut].astype(f32)
                if k:
                    passed[b, :, cut] = total.astype(bf16)

                    @pl.when(z > b)
                    def _():
                        down_hop(b, c, 1).start()

                    @pl.when(z < b)
                    def _():
                        down_hop(b, c, 0).start()
                else:
                    fin[:, cut] = (total + base[:, cut]).astype(bf16)
                    for i in range(len(TP_FLIPS)):
                        owner_copy(c, i).start()
                    owner_own(c).start()

        combine(3)
        given(2)
        give_back(1)
        combine(2)
        given(1)
        give_back(0)
        combine(1)
        shared_out()
        combine(0)

        for c in range(len(cuts)):
            for i in range(len(TP_FLIPS)):
                _, t2 = mate(0, TP_FLIPS[i])
                remote(
                    fin.at[0:rows_each, cuts[c]],
                    out_ref.at[:, pl.ds(pl.multiple_of(t2 * quarter + 128 * c, 128), 128)],
                    f_send.at[c, i], f_recv.at[c, i], at(z, x, t2),
                ).wait_recv()
            owner_own(c).wait()

        for step in range(1, planes):
            along(step).wait_send()
            table_copy(step, 0).wait_send()
        for k in range(planes):
            b = nearest(k)
            across(b).wait_send()
            table_copy(k, 1).wait_send()
            for up in (1, 0):
                @pl.when(goes(b, up))
                def _():
                    z_hop(rblk, b, up, rz_send, rz_recv).wait_send()
                    z_hop(hblk, b, up, hz_send, hz_recv).wait_send()
            for i in range(len(FLIPS)):
                deal_copy(b, *resid_path[1:], i).wait_send()
                deal_copy(b, *heads_path[1:], i).wait_send()
                if k == 0:
                    back_copy(b, 0, i).wait_send()
            if k:
                for c in range(len(cuts)):
                    down_hop(b, c, 0).wait_send()
        for i in range(len(TP_FLIPS)):
            sd_copies[i].wait_send()
            gather(i).wait_send()
            inner_copy(i).wait_send()
            for c in range(len(cuts)):
                owner_copy(c, i).wait_send()

    vmem = pl.BlockSpec(memory_space=pltpu.VMEM)
    anywhere = pl.BlockSpec(memory_space=pl.ANY)
    dma = pltpu.SemaphoreType.DMA
    flips, tps = len(FLIPS), len(TP_FLIPS)
    cut_count = quarter // 128
    return pl.pallas_call(
        kernel,
        out_shape=jax.ShapeDtypeStruct((rows_each, model), bf16),
        in_specs=[vmem] * 5 + [anywhere] * 8,
        out_specs=vmem,
        scratch_shapes=[
            pltpu.VMEM((count,) + own_kv.shape, bf16),
            pltpu.VMEM((count,) + own_table.shape, bf16),
            pltpu.VMEM((1, span), f32),
            pltpu.VMEM((1, span), f32),
            pltpu.VMEM((HEAD_SIZE, span), f32),
            pltpu.VMEM((lanes, lanes), bf16),
            pltpu.VMEM((group, lanes), f32),
            pltpu.VMEM((count, capacity, 128), f32),
            pltpu.VMEM((planes, slots, lanes), bf16),
            pltpu.VMEM((tokens, slots), bf16),
            pltpu.VMEM((planes, tokens, quarter), bf16),
            pltpu.VMEM((planes, tokens, features), bf16),
            pltpu.VMEM((planes, slots, quarter), bf16),
            pltpu.VMEM((planes, slots, features), bf16),
            pltpu.VMEM((count, capacity, model), bf16),
            pltpu.VMEM((count, capacity, tp_count * features), bf16),
            pltpu.VMEM((pair, model), bf16),
            pltpu.VMEM((pair, model), bf16),
            pltpu.VMEM((count, capacity, model), bf16),
            pltpu.VMEM((planes, group, capacity, quarter), bf16),
            pltpu.VMEM((planes, tokens, quarter), bf16),
            pltpu.VMEM((2, planes, tokens, quarter), bf16),
            pltpu.VMEM((tokens, quarter), f32),
            pltpu.VMEM((tokens, quarter), bf16),
            pltpu.VMEM((tokens, tp_count * features), bf16),
            pltpu.VMEM((tokens, quarter), bf16),
            pltpu.VMEM((tokens, tp_count * shared_units), bf16),
            pltpu.VMEM((tp_count * shared_units, quarter), bf16),
            pltpu.VMEM(residual.shape, bf16),
            pltpu.VMEM(out_proj.shape, bf16),
            pltpu.VMEM(gate_w.shape, bf16),
            pltpu.VMEM(up_w.shape, bf16),
            pltpu.VMEM(down_w.shape, bf16),
            pltpu.VMEM(shared_gate.shape, bf16),
            pltpu.VMEM(shared_up.shape, bf16),
            dma((7,)),
            dma((3,)),
            dma((2 * planes,)),
            dma((count,)),
            dma((planes,)),
            dma((planes,)),
            dma((count,)),
            dma((2, planes)),
            dma((planes,)),
            dma((planes, flips)),
            dma((planes, flips + 1)),
            dma((2, planes)),
            dma((planes,)),
            dma((planes, flips)),
            dma((planes, flips + 1)),
            dma((tps,)),
            dma((tps + 1,)),
            dma((tps,)),
            dma((tps + 1,)),
            dma((tps,)),
            dma((tps,)),
            dma((planes, flips)),
            dma((planes, flips + 1)),
            dma((planes, cut_count)),
            dma((2, planes, cut_count)),
            dma((cut_count, tps)),
            dma((cut_count, tps + 1)),
        ],
        compiler_params=pltpu.CompilerParams(
            collective_id=call_id, has_side_effects=True, vmem_limit_bytes=63 * 1024 * 1024
        ),
        name="whole_layer",
    )(queries_t, own_kv, own_table, gain, ffn_gain, residual, *weights)


def scan_attention(query_rows, key_blocks, score_scale):
    start_state = (
        jnp.full((query_rows.shape[0],), -1e30, jnp.float32),
        jnp.zeros((query_rows.shape[0],), jnp.float32),
        jnp.zeros(query_rows.shape, jnp.float32),
    )

    def step(carry, key_slab):
        run_max, run_total, run_acc = carry
        scores = (
            lax.dot_general(
                query_rows,
                key_slab[:, :HEAD_SIZE],
                (((1,), (1,)), ((), ())),
                preferred_element_type=jnp.float32,
            )
            * score_scale
        )
        new_max = jnp.maximum(run_max, jnp.max(scores, axis=1))
        factor = jnp.exp(run_max - new_max)
        expo_terms = jnp.exp(scores - new_max[:, None])
        new_total = run_total * factor + jnp.sum(expo_terms, axis=1)
        new_acc = run_acc * factor[:, None] + jnp.dot(
            expo_terms.astype(jnp.bfloat16),
            key_slab[:, HEAD_SIZE:],
            preferred_element_type=jnp.float32,
        )
        return ((new_max, new_total, new_acc), None)

    (_, run_total, run_acc), _ = lax.scan(step, start_state, key_blocks)
    return run_acc / run_total[:, None]


def slot_ranks(member):
    order = jnp.arange(member.shape[0], dtype=jnp.int32)
    before = (order[:, None] > order[None, :]).astype(jnp.bfloat16)
    rank = jnp.dot(before, member.astype(jnp.bfloat16), preferred_element_type=jnp.float32)
    return jnp.where(member, rank.astype(jnp.int32), -1)


def expert_block(flat_rows, gate_local, up_local, down_local):
    gate_out = jnp.dot(flat_rows, gate_local, preferred_element_type=jnp.float32)
    up_out = jnp.dot(flat_rows, up_local, preferred_element_type=jnp.float32)
    expert_inner = (jax.nn.silu(gate_out) * up_out).astype(jnp.bfloat16)
    return jnp.dot(expert_inner, down_local, preferred_element_type=jnp.float32).astype(
        jnp.bfloat16
    )


def local(
    queries,
    key_matrix,
    values,
    query_gain,
    key_norm_gain,
    head_gain,
    out_proj,
    residual,
    ffn_gain,
    routes,
    route_weights,
    expert_gate,
    expert_up,
    expert_down,
    shared_gate,
    shared_up,
    shared_down,
):
    tok_count = queries.shape[0]
    head_count = queries.shape[1] // HEAD_SIZE
    sp_count = lax.axis_size("sp")
    tp_count = lax.axis_size("tp")
    tp_index = lax.axis_index("tp")
    sequence_total = tok_count * sp_count
    positions = lax.axis_index("sp") * tok_count + jnp.arange(tok_count, dtype=jnp.int32)
    cosine_table, sine_table = grid_tables(positions, sequence_total)
    rotated_query = apply_rotary(
        final_norm(
            queries.astype(jnp.float32).reshape(tok_count, head_count, HEAD_SIZE), query_gain
        ),
        cosine_table,
        sine_table,
    ).astype(jnp.bfloat16)
    rotated_key = (
        apply_rotary(
            final_norm(
                key_matrix.astype(jnp.float32).reshape(tok_count, 1, HEAD_SIZE), key_norm_gain
            ),
            cosine_table,
            sine_table,
        )
        .reshape(tok_count, HEAD_SIZE)
        .astype(jnp.bfloat16)
    )
    packed = jnp.concatenate([rotated_key, values], axis=1)
    score_scale = HEAD_SIZE ** (-0.5)
    topk_count = routes.shape[1]
    capacity = max(2, 2 * tok_count * topk_count // (sp_count * tp_count))
    lanes = 2 * HEAD_SIZE
    entries = tok_count * topk_count
    relayed = (
        tp_count == 4
        and sp_count == 2 * tp_count
        and capacity % 16 == 0
        and tok_count % (16 * tp_count) == 0
        and entries % lanes == 0
        and head_count * tok_count % 256 == 0
        and head_count % 2 == 0
    )
    if relayed:
        lane_total = -(-tok_count // 128) * 128
        scale_hi = lax.reduce_precision(route_weights, 8, 7)
        tables = jnp.concatenate(
            [routes.astype(jnp.float32), scale_hi, route_weights - scale_hi], axis=1
        ).T
        tables = jnp.pad(
            tables, ((0, -3 * topk_count % 16), (0, lane_total - tok_count)), constant_values=-1.0
        ).astype(jnp.bfloat16)
        tables = tables.reshape(tables.shape[0], -1, 128).transpose(1, 0, 2).reshape(-1, 128)
        scaled = rotated_query * jnp.asarray(score_scale, jnp.bfloat16)
        return whole_layer(
            scaled.transpose(2, 1, 0).reshape(HEAD_SIZE, head_count * tok_count),
            packed,
            tables,
            head_gain.reshape(1, -1),
            ffn_gain.reshape(1, -1),
            residual,
            (out_proj, expert_gate[0], expert_up[0], expert_down[0], shared_gate, shared_up, shared_down),
            tok_count,
            capacity,
            topk_count,
            sp_count // tp_count,
            tp_count,
            0,
        )
    piece = exchange(packed, "sp", 0, True).reshape(sequence_total, lanes)
    query_rows = rotated_query.transpose(1, 0, 2).reshape(head_count * tok_count, HEAD_SIZE)
    block_length = key_block_rows(sequence_total)
    key_blocks = piece.reshape(sequence_total // block_length, block_length, lanes)
    attended = scan_attention(query_rows, key_blocks, score_scale)
    attended = attended.reshape(head_count, tok_count, HEAD_SIZE).transpose(1, 0, 2)
    head_out = final_norm(attended, head_gain.reshape(head_count, HEAD_SIZE))
    head_out = head_out.astype(jnp.bfloat16).reshape(tok_count, head_count * HEAD_SIZE)
    part_rows = tok_count // tp_count
    token_heads = exchange(
        head_out.reshape(tp_count, part_rows, head_count * HEAD_SIZE), "tp", 1, False
    )
    token_heads = token_heads.transpose(1, 0, 2).reshape(part_rows, -1)
    own_resid = lax.dynamic_slice_in_dim(residual, tp_index * part_rows, part_rows, 0)
    hidden_own = (
        own_resid.astype(jnp.float32)
        + jnp.dot(token_heads, out_proj, preferred_element_type=jnp.float32)
    ).astype(jnp.bfloat16)
    normed_own = final_norm(hidden_own.astype(jnp.float32), ffn_gain).astype(jnp.bfloat16)
    model_width = normed_own.shape[1]
    gate_local = expert_gate[0]
    up_local = expert_up[0]
    down_local = expert_down[0]
    normed = exchange(normed_own, "tp", 2, True).reshape(tok_count, model_width)
    slot_total = sp_count * capacity
    experts_here = jnp.arange(sp_count, dtype=jnp.int32) * tp_count + tp_index
    named = routes[:, :, None] == experts_here[None, None, :]
    member = jnp.any(named, axis=1)
    scale = jnp.sum(jnp.where(named, route_weights[:, :, None], 0.0), axis=1)
    rank = slot_ranks(member)
    slots = jnp.arange(capacity, dtype=jnp.int32)
    chosen = rank.T[:, None, :] == slots[None, :, None]
    select = chosen.astype(jnp.bfloat16).reshape(slot_total, tok_count)
    outgoing = jnp.dot(select, normed, preferred_element_type=jnp.float32).astype(jnp.bfloat16)
    arrived = exchange(outgoing.reshape(sp_count, capacity, model_width), "sp", 3, False)
    produced = expert_block(
        arrived.reshape(slot_total, model_width), gate_local, up_local, down_local
    )
    returned = exchange(produced.reshape(sp_count, capacity, model_width), "sp", 4, False).reshape(
        slot_total, model_width
    )
    combine = jnp.where(chosen, scale.T[:, None, :], 0.0).reshape(slot_total, tok_count)
    combine_hi = lax.reduce_precision(combine, 8, 7)
    combine_lo = (combine - combine_hi).astype(jnp.bfloat16)
    combine_hi = combine_hi.astype(jnp.bfloat16)

    def mix(weights):
        return lax.dot_general(
            weights, returned, (((0,), (0,)), ((), ())), preferred_element_type=jnp.float32
        )

    gate_part = jnp.dot(normed, shared_gate, preferred_element_type=jnp.float32)
    up_part = jnp.dot(normed, shared_up, preferred_element_type=jnp.float32)
    shared_inner = (jax.nn.silu(gate_part) * up_part).astype(jnp.bfloat16)
    shares = (
        jnp.dot(shared_inner, shared_down, preferred_element_type=jnp.float32)
        + mix(combine_hi)
        + mix(combine_lo)
    ).astype(jnp.bfloat16)
    shares = exchange(shares.reshape(tp_count, part_rows, model_width), "tp", 5, False)
    mixed_rows = jnp.sum(shares.astype(jnp.float32), axis=0)
    return (hidden_own.astype(jnp.float32) + mixed_rows).astype(jnp.bfloat16)


def solution(mesh):
    placed = (
        P("sp", "tp"),
        P("sp", "tp"),
        P("sp", "tp"),
        P(),
        P(),
        P("tp"),
        P(),
        P("sp", None),
        P(),
        P("sp", None),
        P("sp", None),
        P(("sp", "tp"), None, None),
        P(("sp", "tp"), None, None),
        P(("sp", "tp"), None, None),
        P(None, "tp"),
        P(None, "tp"),
        P("tp", None),
    )
    return jax.shard_map(
        local, mesh=mesh, in_specs=placed, out_specs=P(("sp", "tp"), None), check_vma=False
    )
```
